512 devices in a mesh: kv: 128 (over z, y, core), tp: 4 (over x).
Axes of the slice: x: 4, y: 8, z: 8, core: 2. Of those that a mesh axis runs over, the one named last changes fastest.
Arguments:
- hidden: bfloat16 [128, 4096], P(None, 'tp'), may hold values from -50 to 50
- input_gain: bfloat16 [4096], P('tp'), may hold values from 0.099609375 to 1.8984375
- x_weight: bfloat16 [4096, 8192], P('tp', 'kv'), may hold values from -0.09375 to 0.09375
- z_weight: bfloat16 [4096, 8192], P('tp', 'kv'), may hold values from -0.09375 to 0.09375
- bc_weight: bfloat16 [4096, 8192], P('tp', 'kv'), may hold values from -0.09375 to 0.09375
- dt_weight: bfloat16 [4096, 128], P('tp', 'kv'), may hold values from -0.09375 to 0.09375
- x_kernel: bfloat16 [4, 8192], P(None, 'kv'), may hold values from -3 to 3
- bc_kernel: bfloat16 [4, 8192], P(None, 'kv'), may hold values from -3 to 3
- dt_bias: float32 [128], P('kv'), may hold values from -3 to 0.5
- decay_log: float32 [128], P('kv'), may hold values from -3 to 1.5
- skip_scale: float32 [128], P('kv'), may hold values from 0.5 to 1.5
- output_gain: bfloat16 [8192], P('kv'), may hold values from 0.099609375 to 1.8984375
- output_weight: bfloat16 [8192, 4096], P('kv'), may hold values from -0.25 to 0.25
- saved_states: float32 [32, 5, 128, 64, 128], P('tp', None, 'kv'), may hold values from -1.8 to 1.8
- x_history: bfloat16 [32, 7, 8192], P('tp', None, 'kv'), may hold values from -6 to 6
- bc_history: bfloat16 [32, 7, 8192], P('tp', None, 'kv'), may hold values from -6 to 6
- accepted: int32 [32], P('tp'), may hold values from 0 to 4
Outputs:
- mixed: bfloat16 [128, 4096], P('tp', 'kv')
- new_states: float32 [32, 5, 128, 64, 128], P('tp', None, 'kv')
- x_window: bfloat16 [32, 7, 8192], P('tp', None, 'kv')
- bc_window: bfloat16 [32, 7, 8192], P('tp', None, 'kv')
The draws below stay inside these ranges and needn't reach their ends.
All inputs are finite; a program needn't handle non-finite values.
Results may differ from the reference program's by a relative error of at most 0.02.
Values may be sent and summed in bfloat16 or wider, within the bound.
A program may use at most 64 MiB of HBM per device.

```python
import jax
import jax.numpy as jnp
from jax import lax

D = 4096
HEADS = 128
HEAD_SIZE = 64
STATE = 128
GROUPS = 32
CONV = 4
PROPS = 4
SEQS = 32
TOKENS = 128
INNER = 8192
BC_WIDTH = 8192
HIST = 7
FEATURE_BLOCKS = 4


def draw_hidden(key, part):
    noise_key = jax.random.fold_in(key, 0)
    samples = jnp.clip(jax.random.normal(noise_key, (TOKENS, D), jnp.float32), -6.0, 6.0)
    quarter = jnp.arange(D) * 4 // D
    factors = jnp.array([0.5, 1.6, 0.4, 1.2], jnp.float32)[quarter]
    return (samples * factors[None, :]).astype(jnp.bfloat16)


def set_ends(result, rng, smallest, top_value):
    longest = result.shape.index(max(result.shape))
    spots = []
    for shift in (0, 1):
        where = [jax.random.randint(jax.random.fold_in(rng, axis), (), 0, length) for axis, length in enumerate(result.shape)]
        where[longest] = (where[longest] + shift) % result.shape[longest]
        spots.append(tuple(where))
    return result.at[spots[0]].set(smallest).at[spots[1]].set(top_value)


def with_spikes(entries, rng, source, target, shards_of, factor):
    owner, partner = [(jnp.arange(entries.shape[dim]) // (entries.shape[dim] // shards_of)).reshape([-1 if axis == dim else 1 for axis in range(entries.ndim)]) for dim in (source, target)]
    chosen = jax.random.permutation(rng, shards_of)[partner]
    strong = (owner == chosen) | (owner == (partner + shards_of // 2) % shards_of)
    return jnp.where(strong, factor * entries, entries)


def level_of(rng, extent, shards, low, top_value):
    gain = 1.0
    for axis_at, blocks in shards:
        draws = jax.random.uniform(jax.random.fold_in(jax.random.fold_in(rng, 6), axis_at), (blocks,), jnp.float32, low / len(shards), top_value / len(shards))
        gain = gain * jnp.repeat(jnp.exp(draws), extent[axis_at] // blocks).reshape((-1,) + (1,) * (len(extent) - 1 - axis_at))
    return gain


def bell_draw(key, dims, width, limit, cuts=(), kind=jnp.bfloat16):
    gain = level_of(key, dims, cuts, -0.22, 0.18) if cuts else 1.0
    values = jax.random.normal(key, dims, jnp.float32) * width * gain
    return jnp.minimum(jnp.maximum(values, -limit), limit).astype(kind)


def noise_with(stream_key, extent, spread, reach, cuts, heavy, kind=jnp.bfloat16):
    result = spread * jax.random.normal(stream_key, extent, jnp.float32)
    if cuts:
        result = result * level_of(stream_key, extent, cuts, -0.22, 0.18)
    return jnp.clip(with_spikes(result, jax.random.fold_in(stream_key, 3), *heavy), -reach, reach).astype(kind)


def setup_inputs(seed: int = 0) -> dict:
    streams_of = jax.random.split(jax.random.key(seed), 18)
    return {
        "hidden": draw_hidden(jax.random.fold_in(streams_of[17], 71), 0),
        "input_gain": jnp.clip(1.0 + 0.18 * jax.random.normal(streams_of[1], (D,), jnp.float32), 0.099609375, 1.8984375).astype(jnp.bfloat16),
        "x_weight": bell_draw(streams_of[2], (D, INNER), D ** -0.5, 0.09375, ((0, 4), (1, 128))),
        "z_weight": bell_draw(streams_of[3], (D, INNER), D ** -0.5, 0.09375, ((0, 4), (1, 128))),
        "bc_weight": bell_draw(streams_of[4], (D, BC_WIDTH), D ** -0.5, 0.09375, ((0, 4), (1, 128))),
        "dt_weight": bell_draw(streams_of[5], (D, HEADS), D ** -0.5, 0.09375, ((0, 4), (1, 128))),
        "x_kernel": bell_draw(streams_of[6], (CONV, INNER), CONV ** -0.5, 3.0, ((1, 128),)),
        "bc_kernel": bell_draw(streams_of[7], (CONV, BC_WIDTH), CONV ** -0.5, 3.0, ((1, 128),)),
        "dt_bias": jnp.clip(-3.0 + 3.5 * jax.random.uniform(streams_of[8], (HEADS,), jnp.float32) ** level_of(streams_of[8], (HEADS,), ((0, 128),), -0.2, 0.2), -3.0, 0.5),
        "decay_log": jnp.clip(-3.0 + 4.5 * jax.random.uniform(streams_of[9], (HEADS,), jnp.float32) ** level_of(streams_of[9], (HEADS,), ((0, 128),), -0.2, 0.2), -3.0, 1.5),
        "skip_scale": jnp.clip(0.5 + 1.0 * jax.random.uniform(streams_of[10], (HEADS,), jnp.float32) ** level_of(streams_of[10], (HEADS,), ((0, 128),), -0.2, 0.2), 0.5, 1.5),
        "output_gain": jnp.clip(1.0 + 0.18 * jax.random.normal(streams_of[11], (INNER,), jnp.float32), 0.099609375, 1.8984375).astype(jnp.bfloat16),
        "output_weight": noise_with(streams_of[12], (INNER, D), INNER ** -0.5, 0.25, ((0, 128),), (0, 1, 128, 5.5)),
        "saved_states": bell_draw(streams_of[13], (SEQS, PROPS + 1, HEADS, HEAD_SIZE, STATE), 0.3, 1.8, ((0, 4), (2, 128)), jnp.float32),
        "x_history": bell_draw(streams_of[14], (SEQS, HIST, INNER), 1.0, 6.0, ((0, 4), (2, 128))),
        "bc_history": bell_draw(streams_of[15], (SEQS, HIST, BC_WIDTH), 1.0, 6.0, ((0, 4), (2, 128))),
        "accepted": set_ends(jax.random.randint(streams_of[16], (SEQS,), 0, PROPS + 1), jax.random.fold_in(streams_of[16], 1), 0, PROPS).astype(jnp.int32),
    }


EPSILON = 1e-05

def take_window(history, accepted, fresh_rows):
    history_len = history.shape[1] - fresh_rows.shape[1]
    indices = accepted[:, None] + jnp.arange(history_len, dtype=jnp.int32)[None, :]
    kept_rows = jnp.take_along_axis(history, indices[:, :, None], axis=1)
    return jnp.concatenate([kept_rows, fresh_rows], axis=1)

def conv_silu(window, kernel):
    length = window.shape[1] - kernel.shape[0] + 1
    running = window[:, 0:length].astype(jnp.float32) * kernel[0].astype(jnp.float32)
    for offset in range(1, kernel.shape[0]):
        running = running + window[:, offset:offset + length].astype(jnp.float32) * kernel[offset].astype(jnp.float32)
    return jax.nn.silu(running)

def ssd_block(x_conv, step_size, decay_rate, b_terms, c_terms, first_state, skip_scale):
    cumulated = jnp.cumsum(-decay_rate * step_size, axis=1)
    length = x_conv.shape[1]
    indices = jnp.arange(length)
    causal = indices[:, None] >= indices[None, :]
    gaps = cumulated[:, :, None, :] - cumulated[:, None, :, :]
    weights = jnp.exp(jnp.where(causal[None, :, :, None], gaps, -jnp.inf))
    inputs = x_conv * step_size[..., None]
    outer_prod = jnp.einsum('srhp,srhn->srhpn', inputs, b_terms)
    states = jnp.exp(cumulated)[..., None, None] * first_state[:, None] + jnp.einsum('strh,srhpn->sthpn', weights, outer_prod)
    output = jnp.einsum('sthn,sthpn->sthp', c_terms, states) + skip_scale[:, None] * x_conv
    return (output, states)

def reference(hidden, input_gain, x_weight, z_weight, bc_weight, dt_weight, x_kernel, bc_kernel, dt_bias, decay_log, skip_scale, output_gain, output_weight, saved_states, x_history, bc_history, accepted):
    widened = hidden.astype(jnp.float32)
    normed = (widened * lax.rsqrt(lax.optimization_barrier(jnp.mean(widened * widened, axis=1, keepdims=True)) + EPSILON) * input_gain.astype(jnp.float32)).astype(jnp.bfloat16)
    weights = jnp.concatenate([x_weight, z_weight, bc_weight, dt_weight], axis=1)
    feature_block = D // FEATURE_BLOCKS
    running = jnp.zeros((normed.shape[0], weights.shape[1]), jnp.float32)
    for part_index in range(FEATURE_BLOCKS):
        product = jnp.dot(normed[:, part_index * feature_block:(part_index + 1) * feature_block], weights[part_index * feature_block:(part_index + 1) * feature_block], preferred_element_type=jnp.float32)
        running = running + lax.optimization_barrier(product.astype(jnp.bfloat16)).astype(jnp.float32)
    projected = running.astype(jnp.bfloat16)
    x_fresh = projected[:, :INNER]
    z_fresh = projected[:, INNER:2 * INNER]
    bc_fresh = projected[:, 2 * INNER:2 * INNER + BC_WIDTH]
    dt_fresh = projected[:, 2 * INNER + BC_WIDTH:]
    x_window = take_window(x_history, accepted, x_fresh.reshape(SEQS, PROPS, INNER))
    bc_window = take_window(bc_history, accepted, bc_fresh.reshape(SEQS, PROPS, BC_WIDTH))
    x_conv = conv_silu(x_window, x_kernel).reshape(SEQS, PROPS, HEADS, HEAD_SIZE)
    bc_conv = conv_silu(bc_window, bc_kernel).reshape(SEQS, PROPS, GROUPS, 2, STATE)
    b_terms = jnp.repeat(bc_conv[:, :, :, 0], HEADS // GROUPS, axis=2)
    c_terms = jnp.repeat(bc_conv[:, :, :, 1], HEADS // GROUPS, axis=2)
    step_size = jax.nn.softplus(dt_fresh.astype(jnp.float32).reshape(SEQS, PROPS, HEADS) + dt_bias)
    first_state = jnp.take_along_axis(saved_states, accepted[:, None, None, None, None], axis=1)[:, 0]
    decay_rate = jnp.exp(decay_log)

    def one_sequence(pieces):
        x_one, step_one, b_one, c_one, state_one = pieces
        out_one, states_one = ssd_block(x_one[None], step_one[None], decay_rate, b_one[None], c_one[None], state_one[None], skip_scale)
        return (out_one[0], states_one[0])
    output, states = lax.map(one_sequence, (x_conv, step_size, b_terms, c_terms, first_state))
    new_states = jnp.concatenate([first_state[:, None], states], axis=1)
    gate_values = z_fresh.astype(jnp.float32).reshape(SEQS, PROPS, HEADS, HEAD_SIZE)
    gated = (output * jax.nn.silu(gate_values)).reshape(TOKENS, INNER)
    scaled = (gated * output_gain.astype(jnp.float32)).astype(jnp.bfloat16)
    branch = jnp.dot(scaled, output_weight, preferred_element_type=jnp.float32)
    mixed = (lax.rsqrt(lax.optimization_barrier(jnp.mean(gated * gated, axis=1)) + EPSILON)[:, None] * branch).astype(jnp.bfloat16)
    return (mixed, new_states, x_window, bc_window)
```

```python
import jax
import jax.numpy as jnp
from jax import lax
from jax.experimental import pallas as pl
from jax.experimental.pallas import tpu as pltpu
from jax.sharding import PartitionSpec as P

D = 4096
INNER = 8192
EPSILON = 1e-05
MESH = pl.DeviceIdType.MESH
F32 = jnp.float32
BF16 = jnp.bfloat16
SIDE = 8
CHIPS = 64
STEPS = sorted(
    ((dz, dy) for dz in range(SIDE) for dy in range(SIDE) if dz or dy),
    key=lambda p: -(min(p[0], SIDE - p[0]) + min(p[1], SIDE - p[1])),
)


def iota(shape, dim):
    return lax.broadcasted_iota(jnp.int32, shape, dim)


def silu(v):
    return v / (1.0 + jnp.exp(-v))


def softplus(v):
    return jnp.maximum(v, 0.0) + jnp.log1p(jnp.exp(-jnp.abs(v)))


def wait_for(ref, sem):
    pltpu.make_async_copy(ref, ref, sem).wait()


def transpose_blocks(rows):
    lane = iota((8, 128), 1)
    low = lane < 64
    even = lax.rem(lane, 64) < 32
    half = [None] * 4
    for g in range(2):
        near, far = rows[g], rows[g + 2]
        half[g] = jnp.where(low, near, pltpu.roll(far, 64, 1))
        half[g + 2] = jnp.where(low, pltpu.roll(near, 64, 1), far)
    out = []
    for g in (0, 2):
        near, far = half[g], half[g + 1]
        out.append(jnp.where(even, near, pltpu.roll(far, 32, 1)))
        out.append(jnp.where(even, pltpu.roll(near, 96, 1), far))
    return out


def mixer(
    hidden, gain, xw, zw, bcw, dtw, xk, bck, ogain, ow, saved, xh, bch,
    accepted_h, dt_bias, decay_log, skip,
    mixed, states, xwin, bcwin,
    hidden_v, gain_v, wt_v, dt_v, xk_v, bck_v, ogain_v, ow_v, saved_v, xh_v, bch_v,
    hg_v, prod_v, fb_v,
    sa, sb, ra, rb, hs, hr,
    pb, pr, ob, ro, qs, qr, qp, rq, ms,
    accepted, load, sa_s, sb_s, hs_s, ra_s, rb_s, hr_s, pb_s, pr_s, qs_s, qr_s, ob_s, ro_s, qp_s, rq_s, ready,
):
    kv = lax.axis_index("kv")
    tp = lax.axis_index("tp")
    core = lax.rem(kv, 2)
    chip = lax.div(kv, 2)
    y = lax.rem(chip, SIDE)
    z = lax.div(chip, SIDE)
    member = lax.rem(kv, 4)
    base = kv - member

    loads = []

    def fetch(src, dst):
        copy = pltpu.make_async_copy(src, dst, load.at[len(loads)])
        copy.start()
        loads.append(copy)
        return copy

    l_hidden = fetch(hidden, hidden_v)
    l_gain = fetch(gain, gain_v)
    l_dt = fetch(dtw, dt_v)
    l_w = [
        fetch(xw, wt_v.at[pl.ds(0, 64)]),
        fetch(zw, wt_v.at[pl.ds(64, 64)]),
        fetch(bcw, wt_v.at[pl.ds(128, 64)]),
    ]

    barrier = pltpu.get_barrier_semaphore()

    def greet(k, t):
        pl.semaphore_signal(barrier, inc=1, device_id=(k, t), device_id_type=MESH)

    for d in range(1, SIDE):
        greet((lax.rem(z + d, SIDE) * SIDE + y) * 2 + core, tp)
        greet((z * SIDE + lax.rem(y + d, SIDE)) * 2 + core, tp)
    for dm in range(4):
        for dt in range(4):
            if dm or dt:
                greet(base + lax.rem(member + dm, 4), lax.rem(tp + dt, 4))

    l_hist = [fetch(accepted_h, accepted), fetch(xh, xh_v), fetch(bch, bch_v), fetch(xk, xk_v), fetch(bck, bck_v)]
    l_saved = fetch(saved, saved_v)
    l_ow = fetch(ow, ow_v)
    l_ogain = fetch(ogain, ogain_v)

    wt_v[pl.ds(192, 64), :] = jnp.zeros((64, 1024), BF16)
    l_gain.wait()
    l_hidden.wait()
    l_dt.wait()
    gains = gain_v[...].astype(F32)
    gain_row = jnp.concatenate([gains[j : j + 1] for j in range(8)], axis=1)
    dt_row = dt_v[...].astype(F32)
    squares, dts = [], []
    for i in range(4):
        wide = hidden_v[pl.ds(32 * i, 32), :].astype(F32)
        squares.append(jnp.sum(wide * wide, axis=1, keepdims=True))
        gained = (wide * gain_row).astype(BF16)
        hg_v[pl.ds(32 * i, 32), :] = gained
        dts.append(jnp.sum(gained.astype(F32) * dt_row, axis=1, keepdims=True))
    for copy in l_w:
        copy.wait()
    product = lax.dot_general(
        hg_v[...], wt_v[...], (((1,), (1,)), ((), ())), preferred_element_type=F32
    )
    lane32 = iota((32, 128), 1)
    prod_v[0] = product[:, 0:128]
    for i in range(4):
        high = squares[i].astype(BF16).astype(F32)
        tail = product[32 * i : 32 * i + 32, 128:256]
        tail = jnp.where(lane32 == 64, dts[i], tail)
        tail = jnp.where(lane32 == 65, high, tail)
        tail = jnp.where(lane32 == 66, squares[i] - high, tail)
        prod_v[1, pl.ds(32 * i, 32), :] = tail
    for i in range(4):
        for part, out in ((0, sa), (1, sb)):
            rows = [prod_v[part, pl.ds(32 * i + t, 8, stride=4), :] for t in range(4)]
            out[i] = jnp.concatenate(rows, axis=0).astype(BF16)

    for copy in l_hist:
        copy.wait()
    seq = iota((8, 64), 0)
    acc = jnp.zeros((8, 64), jnp.int32)
    for s in range(8):
        acc = jnp.where(seq == s, accepted[s], acc)

    def kept(history):
        wide = [history[i].astype(F32) for i in range(7)]
        out = []
        for j in range(3):
            row = wide[j]
            for k in range(1, 5):
                row = jnp.where(acc == k, wide[j + k], row)
            out.append(row)
        return out

    x_kept = kept(xh_v)
    bc_kept = kept(bch_v)
    packed = jnp.concatenate([*bc_kept, bck_v[...].astype(F32), jnp.zeros((4, 64), F32)], axis=0)
    packed = jnp.concatenate([packed, jnp.zeros((32, 64), F32)], axis=1).astype(BF16)
    hs[...] = packed
    hr[member] = packed
    rb[4 * member] = sb[tp]

    pl.semaphore_wait(barrier, 29)
    for d in range(1, SIDE):
        pl.semaphore_signal(
            ready,
            inc=1,
            device_id=((lax.rem(z + d, SIDE) * SIDE + y) * 2 + core, tp),
            device_id_type=MESH,
        )

    def send(src, dst, send_sem, recv_sem, k, t):
        copy = pltpu.make_async_remote_copy(
            src_ref=src,
            dst_ref=dst,
            send_sem=send_sem,
            recv_sem=recv_sem,
            device_id=(k, t),
            device_id_type=MESH,
        )
        copy.start()
        return copy

    for dt in (2, 1, 3, 0):
        to_t = lax.rem(tp + dt, 4)
        for dm in (2, 3, 1, 0):
            to_k = base + lax.rem(member + dm, 4)
            if dm or dt:
                send(sb.at[to_t], rb.at[4 * member + (4 - dt) % 4], sb_s, rb_s, to_k, to_t)
        if dt:
            send(sa.at[to_t], ra.at[4 - dt], sa_s, ra_s, kv, to_t)
    for dm in (2, 3, 1):
        send(hs, hr.at[member], hs_s, hr_s, base + lax.rem(member + dm, 4), tp)

    l_saved.wait()
    for s in range(8):
        first = saved_v[s, accepted[s]]
        states[s, 0] = first
        fb_v[pl.ds(64 * s, 64), :] = first.astype(BF16)
    l_ogain.wait()
    l_ow.wait()

    wait_for(ra.at[pl.ds(1, 3)], ra_s)
    wait_for(rb.at[pl.ds(0, 15)], rb_s)
    wait_for(hr.at[pl.ds(0, 3)], hr_s)

    def total(blocks):
        out = blocks[0].astype(F32)
        for block in blocks[1:]:
            out = out + block.astype(F32)
        return out

    own = total([rb[4 * member + i] for i in range(4)])
    square_sum = own[:, 65:66] + own[:, 66:67]
    scale = jnp.broadcast_to(lax.rsqrt(square_sum / D + EPSILON), (32, 128))
    xz = (total([sa[tp]] + [ra[i] for i in range(1, 4)]) * scale).astype(BF16).astype(F32)
    dt_fresh = (own * scale).astype(BF16).astype(F32)[:, 64:65]
    fresh = [
        (total([rb[4 * m + i] for i in range(4)]) * scale).astype(BF16).astype(F32)[:, 0:64]
        for m in range(4)
    ]
    stored = [hr[m].astype(F32)[:, 0:64] for m in range(4)]

    def conv(rows, taps):
        out = []
        for t in range(4):
            value = rows[t] * taps[0:1]
            for j in range(1, 4):
                value = value + rows[t + j] * taps[j : j + 1]
            out.append(silu(value))
        return out

    def pieces(value):
        return [value[8 * t : 8 * t + 8] for t in range(4)]

    x_rows = x_kept + pieces(xz[:, 0:64])
    x_conv = conv(x_rows, xk_v[...].astype(F32))
    terms = []
    for low, high in ((0, 1), (2, 3)):
        new = pieces(jnp.concatenate([fresh[low], fresh[high]], axis=1))
        old = jnp.concatenate([stored[low], stored[high]], axis=1)
        taps = old[24:28]
        terms.append(conv(pieces(old)[:3] + new, taps))
    b_terms, c_terms = terms

    rate = jnp.exp(jnp.full((8, 128), decay_log[0], F32))
    steps = pieces(softplus(jnp.broadcast_to(dt_fresh, (32, 128)) + dt_bias[0]))
    cumulated = []
    for t in range(4):
        value = -rate * steps[t]
        cumulated.append(value if t == 0 else cumulated[-1] + value)

    reads = lax.dot_general(
        jnp.concatenate(c_terms, axis=0).astype(BF16),
        fb_v[...],
        (((1,), (1,)), ((), ())),
        preferred_element_type=F32,
    )
    which = lax.rem(iota((32, 128), 0), 8) - jnp.where(lane32 < 64, 0, 1)
    picked = jnp.where(which == 0, reads[:, 0:128], 0.0)
    for i in range(1, 4):
        picked = picked + jnp.where(which == 2 * i, reads[:, 128 * i : 128 * i + 128], 0.0)
    first_part = pieces(picked[:, 0:64] + picked[:, 64:128])

    gated = []
    z_rows = pieces(xz[:, 64:128])
    for t in range(4):
        value = jnp.exp(cumulated[t])[:, 0:64] * first_part[t] + skip[0] * x_conv[t]
        for r in range(t + 1):
            weight = jnp.exp(cumulated[t] - cumulated[r]) * steps[r] if r < t else steps[r]
            inner = jnp.sum(c_terms[t] * b_terms[r], axis=1, keepdims=True)
            value = value + weight[:, 0:64] * inner * x_conv[r]
        gated.append(value * silu(z_rows[t]))
    gated = jnp.concatenate(gated, axis=0)
    square_sum = jnp.sum(gated * gated, axis=1, keepdims=True)
    diagonal = iota((32, 128), 0) == lane32
    row = jnp.sum(jnp.where(diagonal, square_sum, 0.0), axis=0, keepdims=True)
    qs[...] = row
    partner = kv + 1 - 2 * core
    send(qs, qr, qs_s, qr_s, partner, tp)
    scaled = (gated * ogain_v[...].astype(F32)).astype(BF16)

    for k in range(4):
        for n in range(2 * k, 2 * k + 2):
            partial = jnp.dot(
                scaled, ow_v[:, 512 * n : 512 * n + 512], preferred_element_type=F32
            )
            for i in range(4):
                tile = partial[:, 128 * i : 128 * i + 128]
                blocks = transpose_blocks(pieces(tile))
                for b in range(4):
                    pb[b % 2, 2 * (4 * n + i) + b // 2] = blocks[b].astype(BF16)
        part = pl.ds(16 * k, 16)
        send(pb.at[1 - core, part], pr.at[part], pb_s.at[k], pr_s.at[k], partner, tp)

    wait_for(qr, qr_s)
    qp[...] = qs[...] + qr[...]
    pl.semaphore_wait(ready, SIDE - 1)

    def at(dz, dy):
        return lax.rem(z + dz, SIDE) * SIDE + lax.rem(y + dy, SIDE)

    for dz, dy in STEPS:
        send(qp, rq.at[dz * SIDE + dy], qp_s, rq_s, at(dz, dy) * 2 + core, tp)
    for k in range(4):
        part = pl.ds(16 * k, 16)
        wait_for(pr.at[part], pr_s.at[k])
        ob[part] = (pb[core, part].astype(F32) + pr[part].astype(F32)).astype(BF16)
    for dz, dy in STEPS:
        to = at(dz, dy)
        send(ob.at[to], ro.at[dz * SIDE + dy], ob_s, ro_s, to * 2 + core, tp)

    x_in = jnp.concatenate([x_conv[t] * steps[t][:, 0:64] for t in range(4)], axis=0)
    x_cols = jnp.transpose(jnp.concatenate([x_in, jnp.zeros((32, 64), F32)], axis=1))
    decays = [jnp.exp(-rate * steps[t]) for t in range(4)]
    for s in range(8):
        state = saved_v[s, accepted[s]]
        for t in range(4):
            i = 8 * t + s
            state = state * decays[t][s : s + 1] + x_cols[0:64, i : i + 1] * b_terms[t][s : s + 1]
            states[s, t + 1] = state
    for j in range(7):
        xwin[j] = x_rows[j].astype(BF16)
    bc_rows = bc_kept + pieces((own * scale).astype(BF16).astype(F32)[:, 0:64])
    for j in range(7):
        bcwin[j] = bc_rows[j].astype(BF16)

    wait_for(rq.at[pl.ds(1, CHIPS - 1)], rq_s)
    squares_row = qp[...] + jnp.sum(rq[pl.ds(1, CHIPS - 1)], axis=0)
    column = jnp.sum(jnp.where(diagonal, squares_row, 0.0), axis=1, keepdims=True)
    factor = lax.rsqrt(column / INNER + EPSILON)
    wait_for(ro.at[pl.ds(1, CHIPS - 1)], ro_s)
    summed = ob[chip].astype(F32) + jnp.sum(ro[pl.ds(1, CHIPS - 1)].astype(F32), axis=0)
    for t in range(4):
        shifted = pltpu.roll(summed, (128 - 32 * t) % 128, 1) if t else summed
        ms[pl.ds(t, 8, stride=4), :] = shifted * factor[8 * t : 8 * t + 8]
    mixed[...] = ms[:, 0:32].astype(BF16)

    wait_for(sa.at[pl.ds(0, 3)], sa_s)
    wait_for(rb.at[pl.ds(0, 15)], sb_s)
    wait_for(hr.at[pl.ds(0, 3)], hs_s)
    wait_for(qs, qs_s)
    for k in range(4):
        wait_for(pr.at[pl.ds(16 * k, 16)], pb_s.at[k])
    wait_for(rq.at[pl.ds(1, CHIPS - 1)], qp_s)
    wait_for(ro.at[pl.ds(1, CHIPS - 1)], ob_s)


def writer(mixed, states, xwin, bcwin, mixed_o, states_o, xwin_o, bcwin_o, sem):
    copies = [
        pltpu.make_async_copy(states.at[pl.ds(2 * i, 2)], states_o.at[pl.ds(2 * i, 2)], sem.at[i])
        for i in range(4)
    ]
    copies.append(pltpu.make_async_copy(mixed, mixed_o, sem.at[4]))
    copies.append(pltpu.make_async_copy(xwin, xwin_o, sem.at[5]))
    copies.append(pltpu.make_async_copy(bcwin, bcwin_o, sem.at[6]))
    for copy in copies:
        copy.start()
    for copy in copies:
        copy.wait()


def local(
    hidden, input_gain, x_weight, z_weight, bc_weight, dt_weight, x_kernel, bc_kernel,
    dt_bias, decay_log, skip_scale, output_gain, output_weight, saved_states, x_history,
    bc_history, accepted,
):
    shapes = [((32, 32), BF16), ((8, 5, 64, 128), F32), ((7, 8, 64), BF16), ((7, 8, 64), BF16)]
    hbm = pl.BlockSpec(memory_space=pltpu.HBM)
    vmem = pl.BlockSpec(memory_space=pltpu.VMEM)
    smem = pl.BlockSpec(memory_space=pltpu.SMEM)
    dma = pltpu.SemaphoreType.DMA
    scratch = [
        ((128, 1024), BF16), ((8, 128), BF16), ((256, 1024), BF16), ((1, 1024), BF16),
        ((4, 64), BF16), ((4, 64), BF16), ((1, 64), BF16), ((64, 4096), BF16),
        ((8, 5, 64, 128), F32), ((7, 8, 64), BF16), ((7, 8, 64), BF16),
        ((128, 1024), BF16), ((2, 128, 128), F32), ((512, 128), BF16),
        ((4, 32, 128), BF16), ((4, 32, 128), BF16), ((4, 32, 128), BF16), ((16, 32, 128), BF16),
        ((32, 128), BF16), ((4, 32, 128), BF16),
        ((2, 64, 8, 128), BF16), ((64, 8, 128), BF16), ((64, 8, 128), BF16), ((64, 8, 128), BF16),
        ((1, 128), F32), ((1, 128), F32), ((1, 128), F32), ((64, 1, 128), F32), ((32, 128), F32),
    ]
    args = [
        hidden, input_gain.reshape(8, 128), x_weight.T, z_weight.T, bc_weight.T, dt_weight.T,
        x_kernel, bc_kernel, output_gain.reshape(1, 64), output_weight,
        saved_states.reshape(8, 5, 64, 128), x_history.transpose(1, 0, 2),
        bc_history.transpose(1, 0, 2), accepted,
    ]
    args = [pltpu.with_memory_space_constraint(arg, pltpu.HBM) for arg in args]
    results = pl.pallas_call(
        mixer,
        name="mixer",
        out_shape=[pltpu.VMEM(shape, dtype) for shape, dtype in shapes],
        in_specs=[hbm] * len(args) + [smem] * 3,
        out_specs=[vmem] * 4,
        scratch_shapes=[pltpu.VMEM(shape, dtype) for shape, dtype in scratch]
        + [pltpu.SMEM((8,), jnp.int32), dma((20,))]
        + [dma(())] * 6
        + [dma((4,)), dma((4,))]
        + [dma(())] * 6
        + [pltpu.SemaphoreType.REGULAR],
        compiler_params=pltpu.CompilerParams(
            collective_id=0, has_side_effects=True, vmem_limit_bytes=24 << 20
        ),
    )(*args, dt_bias, decay_log, skip_scale)
    mixed, states, xwin, bcwin = pl.pallas_call(
        writer,
        name="writer",
        out_shape=[jax.ShapeDtypeStruct(shape, dtype) for shape, dtype in shapes],
        in_specs=[vmem] * 4,
        out_specs=[hbm] * 4,
        scratch_shapes=[dma((7,))],
        compiler_params=pltpu.CompilerParams(vmem_limit_bytes=8 << 20),
    )(*results)
    return (
        mixed,
        states.reshape(8, 5, 1, 64, 128),
        xwin.transpose(1, 0, 2),
        bcwin.transpose(1, 0, 2),
    )


def solution(mesh):
    return jax.shard_map(
        local,
        mesh=mesh,
        in_specs=(
            P(None, "tp"), P("tp"), P("tp", "kv"), P("tp", "kv"), P("tp", "kv"), P("tp", "kv"),
            P(None, "kv"), P(None, "kv"), P("kv"), P("kv"), P("kv"), P("kv"), P("kv", None),
            P("tp", None, "kv", None, None), P("tp", None, "kv"), P("tp", None, "kv"), P("tp"),
        ),
        out_specs=(
            P("tp", "kv"), P("tp", None, "kv", None, None), P("tp", None, "kv"), P("tp", None, "kv"),
        ),
        check_vma=False,
    )
```

```python
import jax
import jax.numpy as jnp
from jax import lax
from jax.experimental import pallas as pl
from jax.experimental.pallas import tpu as pltpu
from jax.sharding import PartitionSpec as P

D = 4096
INNER = 8192
EPSILON = 1e-05
MESH = pl.DeviceIdType.MESH
F32 = jnp.float32
BF16 = jnp.bfloat16
SIDE = 8
FAR = (4, 3, 5, 2, 6, 1, 7, 0)
CORNER = [(dz, dy) for dz in FAR[:3] for dy in FAR[:3]]
OTHERS = sorted(
    ((dz, dy) for dz in FAR for dy in FAR if (dz or dy) and (dz, dy) not in CORNER),
    key=lambda p: -(min(p[0], SIDE - p[0]) + min(p[1], SIDE - p[1])),
)


def iota(shape, dim):
    return lax.broadcasted_iota(jnp.int32, shape, dim)


def silu(v):
    return v / (1.0 + jnp.exp(-v))


def softplus(v):
    return jnp.maximum(v, 0.0) + jnp.log1p(jnp.exp(-jnp.abs(v)))


def wait_for(ref, sem):
    pltpu.make_async_copy(ref, ref, sem).wait()


def transpose_blocks(rows):
    lane = iota((8, 128), 1)
    low = lane < 64
    even = lax.rem(lane, 64) < 32
    half = [None] * 4
    for g in range(2):
        near, far = rows[g], rows[g + 2]
        half[g] = jnp.where(low, near, pltpu.roll(far, 64, 1))
        half[g + 2] = jnp.where(low, pltpu.roll(near, 64, 1), far)
    out = []
    for g in (0, 2):
        near, far = half[g], half[g + 1]
        out.append(jnp.where(even, near, pltpu.roll(far, 32, 1)))
        out.append(jnp.where(even, pltpu.roll(near, 96, 1), far))
    return out


def mixer(
    hidden, gain, xw, zw, bcw, dtw, xk, bck, ogain, ow, saved, xh, bch,
    accepted_h, dt_bias, decay_log, skip,
    mixed, states, xwin, bcwin,
    hidden_v, gain_v, wt_v, dt_v, xk_v, bck_v, ogain_v, ow_v, saved_v, xh_v, bch_v,
    hg_v, prod_v, fb_v,
    sa, sb, ra, rb, hs, hr,
    wk, ws, sx, sr, ob, ro, qs, qr, qp, rq, ms,
    accepted, load, sa_s, sb_s, hs_s, ra_s, rb_s, hr_s, ws_s, wr_s, sx_s, sr_s, qs_s, qr_s, ob_s, ro_s, qp_s, rq_s, near, ready,
):
    kv = lax.axis_index("kv")
    tp = lax.axis_index("tp")
    core = lax.rem(kv, 2)
    chip = lax.div(kv, 2)
    y = lax.rem(chip, SIDE)
    z = lax.div(chip, SIDE)
    member = lax.rem(kv, 4)
    base = kv - member

    def at(dz, dy):
        return (lax.rem(z + dz, SIDE) * SIDE + lax.rem(y + dy, SIDE)) * 2 + core

    loads = []

    def fetch(src, dst):
        copy = pltpu.make_async_copy(src, dst, load.at[len(loads)])
        copy.start()
        loads.append(copy)
        return copy

    l_hidden = fetch(hidden, hidden_v)
    l_gain = fetch(gain, gain_v)
    l_dt = fetch(dtw, dt_v)
    l_w = [
        fetch(xw, wt_v.at[pl.ds(0, 64)]),
        fetch(zw, wt_v.at[pl.ds(64, 64)]),
        fetch(bcw, wt_v.at[pl.ds(128, 64)]),
    ]

    barrier = pltpu.get_barrier_semaphore()

    def greet(k, t):
        pl.semaphore_signal(barrier, inc=1, device_id=(k, t), device_id_type=MESH)

    for dt in (2, 1, 3, 0):
        for dm in (2, 3, 1, 0):
            if dm or dt:
                greet(base + lax.rem(member + dm, 4), lax.rem(tp + dt, 4))
    for d in (3, 5, 2, 6, 1, 7):
        greet(at(d, 0), tp)
        greet(at(0, d), tp)

    l_hist = [fetch(accepted_h, accepted), fetch(xh, xh_v), fetch(bch, bch_v), fetch(xk, xk_v), fetch(bck, bck_v)]
    l_saved = fetch(saved, saved_v)
    l_ow = fetch(ow, ow_v)
    l_ogain = fetch(ogain, ogain_v)

    wt_v[pl.ds(192, 64), :] = jnp.zeros((64, 1024), BF16)
    l_gain.wait()
    l_hidden.wait()
    l_dt.wait()
    gains = gain_v[...].astype(F32)
    gain_row = jnp.concatenate([gains[j : j + 1] for j in range(8)], axis=1)
    dt_row = dt_v[...].astype(F32)
    squares, dts = [], []
    for i in range(4):
        wide = hidden_v[pl.ds(32 * i, 32), :].astype(F32)
        squares.append(jnp.sum(wide * wide, axis=1, keepdims=True))
        gained = (wide * gain_row).astype(BF16)
        hg_v[pl.ds(32 * i, 32), :] = gained
        dts.append(jnp.sum(gained.astype(F32) * dt_row, axis=1, keepdims=True))
    for copy in l_w:
        copy.wait()
    product = lax.dot_general(
        hg_v[...], wt_v[...], (((1,), (1,)), ((), ())), preferred_element_type=F32
    )
    lane32 = iota((32, 128), 1)
    prod_v[0] = product[:, 0:128]
    for i in range(4):
        high = squares[i].astype(BF16).astype(F32)
        tail = product[32 * i : 32 * i + 32, 128:256]
        tail = jnp.where(lane32 == 64, dts[i], tail)
        tail = jnp.where(lane32 == 65, high, tail)
        tail = jnp.where(lane32 == 66, squares[i] - high, tail)
        prod_v[1, pl.ds(32 * i, 32), :] = tail
    lane = iota((8, 128), 1)
    low = lane < 64
    for i in range(4):
        rows = [prod_v[0, pl.ds(32 * i + t, 8, stride=4), :] for t in range(4)]
        tails = [prod_v[1, pl.ds(32 * i + t, 8, stride=4), :] for t in range(4)]
        misc = tails[0]
        for t in range(1, 4):
            misc = jnp.where(lane < 64 + 4 * t, misc, pltpu.roll(tails[t], 4 * t, 1))
        sa[i] = jnp.concatenate([*rows, misc], axis=0).astype(BF16)
        sb[i] = jnp.concatenate(
            [jnp.where(low, tails[t], pltpu.roll(tails[t + 1], 64, 1)) for t in (0, 2)], axis=0
        ).astype(BF16)

    for copy in l_hist:
        copy.wait()
    seq = iota((8, 64), 0)
    acc = jnp.zeros((8, 64), jnp.int32)
    for s in range(8):
        acc = jnp.where(seq == s, accepted[s], acc)

    def kept(history):
        wide = [history[i].astype(F32) for i in range(7)]
        out = []
        for j in range(3):
            row = wide[j]
            for k in range(1, 5):
                row = jnp.where(acc == k, wide[j + k], row)
            out.append(row)
        return out

    x_kept = kept(xh_v)
    bc_kept = kept(bch_v)
    packed = jnp.concatenate([*bc_kept, bck_v[...].astype(F32), jnp.zeros((4, 64), F32)], axis=0)
    packed = jnp.concatenate([packed, jnp.zeros((32, 64), F32)], axis=1).astype(BF16)
    hs[...] = packed
    hr[member] = packed
    rb[4 * member] = sb[tp]

    pl.semaphore_wait(barrier, 27)

    def tell(sem, k):
        pl.semaphore_signal(sem, inc=1, device_id=(k, tp), device_id_type=MESH)

    tell(near, at(7, 0))
    tell(near, at(0, 7))
    def send(src, dst, send_sem, recv_sem, k, t):
        copy = pltpu.make_async_remote_copy(
            src_ref=src,
            dst_ref=dst,
            send_sem=send_sem,
            recv_sem=recv_sem,
            device_id=(k, t),
            device_id_type=MESH,
        )
        copy.start()
        return copy

    for dt in (2, 1, 3, 0):
        to_t = lax.rem(tp + dt, 4)
        for dm in (2, 3, 1, 0):
            to_k = base + lax.rem(member + dm, 4)
            if dm or dt:
                send(sb.at[to_t], rb.at[4 * member + (4 - dt) % 4], sb_s, rb_s, to_k, to_t)
        if dt:
            send(sa.at[to_t], ra.at[4 - dt], sa_s, ra_s, kv, to_t)
    for dm in (2, 3, 1):
        send(hs, hr.at[member], hs_s, hr_s, base + lax.rem(member + dm, 4), tp)

    l_saved.wait()
    for s in range(8):
        first = saved_v[s, accepted[s]]
        states[s, 0] = first
        fb_v[pl.ds(64 * s, 64), :] = first.astype(BF16)
    l_ogain.wait()
    l_ow.wait()
    quarter = lax.div(iota((64, 128), 1), 32)
    flip = core == 1
    for i in range(16):
        left = ow_v[:, 256 * i : 256 * i + 128].astype(F32)
        right = ow_v[:, 256 * i + 128 : 256 * i + 256].astype(F32)
        left_64, right_32 = pltpu.roll(left, 64, 1), pltpu.roll(right, 32, 1)
        left_96, right_64 = pltpu.roll(left, 96, 1), pltpu.roll(right, 64, 1)
        first = jnp.where(quarter < 2, jnp.where(quarter == 0, left, left_96), jnp.where(quarter == 2, right_64, right_32))
        second = jnp.where(quarter < 2, jnp.where(quarter == 0, left_96, left_64), jnp.where(quarter == 2, right_32, right))
        wk[0:64, 128 * i : 128 * i + 128] = jnp.where(flip, second, first).astype(BF16)
        ws[:, 128 * i : 128 * i + 128] = jnp.where(flip, first, second).astype(BF16)
    partner = kv + 1 - 2 * core
    send(ws, wk.at[pl.ds(64, 64)], ws_s, wr_s, partner, tp)
    pl.semaphore_wait(near, 2)
    for d in FAR[:-1]:
        tell(ready, at(d, 0))

    wait_for(ra.at[pl.ds(1, 3)], ra_s)
    wait_for(rb.at[pl.ds(0, 15)], rb_s)
    wait_for(hr.at[pl.ds(0, 3)], hr_s)

    def total(blocks):
        out = blocks[0].astype(F32)
        for block in blocks[1:]:
            out = out + block.astype(F32)
        return out

    def pieces(value):
        return [value[8 * t : 8 * t + 8] for t in range(4)]

    def spread(value, at):
        return jnp.broadcast_to(value[:, at : at + 1], (8, 128))

    def rounded(value):
        return value.astype(BF16).astype(F32)

    wide = total([sa[tp]] + [ra[i] for i in range(1, 4)])
    misc = wide[32:40]
    scales = lax.rsqrt((misc + pltpu.roll(misc, 127, 1)) / D + EPSILON)
    dt_fresh = rounded(misc * pltpu.roll(scales, 127, 1))
    scale = [spread(scales, 65 + 4 * t) for t in range(4)]
    xz = [rounded(wide[8 * t : 8 * t + 8] * scale[t]) for t in range(4)]
    fresh = [total([rb[4 * m + i] for i in range(4)]) for m in range(4)]
    stored = [hr[m].astype(F32)[:, 0:64] for m in range(4)]

    def conv(rows, taps):
        out = []
        for t in range(4):
            value = rows[t] * taps[0:1]
            for j in range(1, 4):
                value = value + rows[t + j] * taps[j : j + 1]
            out.append(silu(value))
        return out

    x_rows = x_kept + [value[:, 0:64] for value in xz]
    x_conv = conv(x_rows, xk_v[...].astype(F32))
    terms = []
    for left, right in ((0, 1), (2, 3)):
        new = []
        for t in (0, 2):
            near, far = (fresh[m][4 * t : 4 * t + 8] for m in (left, right))
            new.append(jnp.where(low, near, pltpu.roll(far, 64, 1)))
            new.append(jnp.where(low, pltpu.roll(near, 64, 1), far))
        new = [rounded(new[t] * scale[t]) for t in range(4)]
        old = jnp.concatenate([stored[left], stored[right]], axis=1)
        terms.append(conv(pieces(old)[:3] + new, old[24:28]))
    b_terms, c_terms = terms

    rate = jnp.exp(jnp.full((8, 128), decay_log[0], F32))
    all_steps = softplus(dt_fresh + dt_bias[0])
    steps = [spread(all_steps, 64 + 4 * t) for t in range(4)]
    cumulated = []
    for t in range(4):
        value = -rate * steps[t]
        cumulated.append(value if t == 0 else cumulated[-1] + value)

    reads = lax.dot_general(
        jnp.concatenate(c_terms, axis=0).astype(BF16),
        fb_v[...],
        (((1,), (1,)), ((), ())),
        preferred_element_type=F32,
    )
    which = lax.rem(iota((32, 128), 0), 8) - jnp.where(lane32 < 64, 0, 1)
    picked = jnp.where(which == 0, reads[:, 0:128], 0.0)
    for i in range(1, 4):
        picked = picked + jnp.where(which == 2 * i, reads[:, 128 * i : 128 * i + 128], 0.0)
    first_part = pieces(picked[:, 0:64] + picked[:, 64:128])

    gated = []
    z_rows = [value[:, 64:128] for value in xz]
    for t in range(4):
        value = jnp.exp(cumulated[t])[:, 0:64] * first_part[t] + skip[0] * x_conv[t]
        for r in range(t + 1):
            weight = jnp.exp(cumulated[t] - cumulated[r]) * steps[r] if r < t else steps[r]
            inner = jnp.sum(c_terms[t] * b_terms[r], axis=1, keepdims=True)
            value = value + weight[:, 0:64] * inner * x_conv[r]
        gated.append(value * silu(z_rows[t]))
    gated = jnp.concatenate(gated, axis=0)
    scaled = (gated * ogain_v[...].astype(F32)).astype(BF16)
    sx[...] = jnp.concatenate([scaled, jnp.zeros((32, 64), BF16)], axis=1)
    send(sx, sr, sx_s, sr_s, partner, tp)
    square_sum = jnp.sum(gated * gated, axis=1, keepdims=True)
    diagonal = iota((32, 128), 0) == lane32
    qs[...] = jnp.sum(jnp.where(diagonal, square_sum, 0.0), axis=0, keepdims=True)
    send(qs, qr, qs_s, qr_s, partner, tp)
    pl.semaphore_wait(ready, SIDE - 1)

    wait_for(qr, qr_s)
    qp[...] = qs[...] + qr[...]
    wait_for(wk.at[pl.ds(64, 64)], wr_s)
    wait_for(sr, sr_s)

    rows = jnp.concatenate([scaled, sr[:, 0:64]], axis=1)

    def multiply(i):
        start = pl.multiple_of(lax.rem(z + FAR[i], SIDE) * 256, 256)
        partial = jnp.dot(rows, wk[:, pl.ds(start, 256)], preferred_element_type=F32)
        for j in range(2):
            blocks = transpose_blocks(pieces(partial[:, 128 * j : 128 * j + 128]))
            for b in range(4):
                ob[i, 4 * j + b] = blocks[b].astype(BF16)

    def spread_out(dz, dy):
        to = at(dz, dy)
        slot = dz * SIDE + dy
        send(ob.at[FAR.index(dz), lax.rem(y + dy, SIDE)], ro.at[slot], ob_s, ro_s, to, tp)
        send(qp, rq.at[slot], qp_s, rq_s, to, tp)

    for i in range(3):
        multiply(i)
    for dz, dy in CORNER:
        spread_out(dz, dy)
    for i in range(3, SIDE):
        multiply(i)
    for dz, dy in OTHERS:
        spread_out(dz, dy)

    x_in = jnp.concatenate([x_conv[t] * steps[t][:, 0:64] for t in range(4)], axis=0)
    x_cols = jnp.transpose(jnp.concatenate([x_in, jnp.zeros((32, 64), F32)], axis=1))
    decays = [jnp.exp(-rate * steps[t]) for t in range(4)]
    for s in range(8):
        state = saved_v[s, accepted[s]]
        for t in range(4):
            i = 8 * t + s
            state = state * decays[t][s : s + 1] + x_cols[0:64, i : i + 1] * b_terms[t][s : s + 1]
            states[s, t + 1] = state
    for j in range(7):
        xwin[j] = x_rows[j].astype(BF16)
    own = total([rb[4 * member + i] for i in range(4)])
    bc_rows = list(bc_kept)
    for t in range(4):
        half = own[8 * (t // 2) : 8 * (t // 2) + 8, 64 * (t % 2) : 64 * (t % 2) + 64]
        bc_rows.append(rounded(half * scale[t][:, 0:64]))
    for j in range(7):
        bcwin[j] = bc_rows[j].astype(BF16)

    wait_for(rq.at[pl.ds(1, 63)], rq_s)
    squares_row = qp[...] + jnp.sum(rq[pl.ds(1, 63)], axis=0)
    column = jnp.sum(jnp.where(diagonal, squares_row, 0.0), axis=1, keepdims=True)
    factor = lax.rsqrt(column / INNER + EPSILON)
    wait_for(ro.at[pl.ds(1, 63)], ro_s)
    summed = ob[7, y].astype(F32) + jnp.sum(ro[pl.ds(1, 63)].astype(F32), axis=0)
    for t in range(4):
        shifted = pltpu.roll(summed, (128 - 32 * t) % 128, 1) if t else summed
        ms[pl.ds(t, 8, stride=4), :] = shifted * factor[8 * t : 8 * t + 8]
    mixed[...] = ms[:, 0:32].astype(BF16)

    wait_for(sa.at[pl.ds(0, 3)], sa_s)
    wait_for(rb.at[pl.ds(0, 15)], sb_s)
    wait_for(hr.at[pl.ds(0, 3)], hs_s)
    wait_for(ws, ws_s)
    wait_for(sx, sx_s)
    wait_for(qs, qs_s)
    wait_for(ro.at[pl.ds(1, 63)], ob_s)
    wait_for(rq.at[pl.ds(1, 63)], qp_s)


def writer(mixed, states, xwin, bcwin, mixed_o, states_o, xwin_o, bcwin_o, sem):
    copies = [
        pltpu.make_async_copy(states.at[pl.ds(2 * i, 2)], states_o.at[pl.ds(2 * i, 2)], sem.at[i])
        for i in range(4)
    ]
    copies.append(pltpu.make_async_copy(mixed, mixed_o, sem.at[4]))
    copies.append(pltpu.make_async_copy(xwin, xwin_o, sem.at[5]))
    copies.append(pltpu.make_async_copy(bcwin, bcwin_o, sem.at[6]))
    for copy in copies:
        copy.start()
    for copy in copies:
        copy.wait()


def local(
    hidden, input_gain, x_weight, z_weight, bc_weight, dt_weight, x_kernel, bc_kernel,
    dt_bias, decay_log, skip_scale, output_gain, output_weight, saved_states, x_history,
    bc_history, accepted,
):
    shapes = [((32, 32), BF16), ((8, 5, 64, 128), F32), ((7, 8, 64), BF16), ((7, 8, 64), BF16)]
    hbm = pl.BlockSpec(memory_space=pltpu.HBM)
    smem = pl.BlockSpec(memory_space=pltpu.SMEM)
    vmem = pl.BlockSpec(memory_space=pltpu.VMEM)
    dma = pltpu.SemaphoreType.DMA
    scratch = [
        ((128, 1024), BF16), ((8, 128), BF16), ((256, 1024), BF16), ((1, 1024), BF16),
        ((4, 64), BF16), ((4, 64), BF16), ((1, 64), BF16), ((64, 4096), BF16),
        ((8, 5, 64, 128), F32), ((7, 8, 64), BF16), ((7, 8, 64), BF16),
        ((128, 1024), BF16), ((2, 128, 128), F32), ((512, 128), BF16),
        ((4, 40, 128), BF16), ((4, 16, 128), BF16), ((4, 40, 128), BF16), ((16, 16, 128), BF16),
        ((32, 128), BF16), ((4, 32, 128), BF16),
        ((128, 2048), BF16), ((64, 2048), BF16), ((32, 128), BF16), ((32, 128), BF16),
        ((8, 8, 8, 128), BF16), ((64, 8, 128), BF16),
        ((1, 128), F32), ((1, 128), F32), ((1, 128), F32), ((64, 1, 128), F32), ((32, 128), F32),
    ]
    args = [
        hidden, input_gain.reshape(8, 128), x_weight.T, z_weight.T, bc_weight.T, dt_weight.T,
        x_kernel, bc_kernel, output_gain.reshape(1, 64), output_weight,
        saved_states.reshape(8, 5, 64, 128), x_history.transpose(1, 0, 2),
        bc_history.transpose(1, 0, 2), accepted,
    ]
    args = [pltpu.with_memory_space_constraint(arg, pltpu.HBM) for arg in args]
    results = pl.pallas_call(
        mixer,
        name="mixer",
        out_shape=[pltpu.VMEM(shape, dtype) for shape, dtype in shapes],
        in_specs=[hbm] * len(args) + [smem] * 3,
        out_specs=[vmem] * 4,
        scratch_shapes=[pltpu.VMEM(shape, dtype) for shape, dtype in scratch]
        + [pltpu.SMEM((8,), jnp.int32), dma((20,))]
        + [dma(())] * 16
        + [pltpu.SemaphoreType.REGULAR] * 2,
        compiler_params=pltpu.CompilerParams(
            collective_id=0, has_side_effects=True, vmem_limit_bytes=24 << 20
        ),
    )(*args, dt_bias, decay_log, skip_scale)
    mixed, states, xwin, bcwin = pl.pallas_call(
        writer,
        name="writer",
        out_shape=[jax.ShapeDtypeStruct(shape, dtype) for shape, dtype in shapes],
        in_specs=[vmem] * 4,
        out_specs=[hbm] * 4,
        scratch_shapes=[dma((7,))],
        compiler_params=pltpu.CompilerParams(vmem_limit_bytes=8 << 20),
    )(*results)
    return (
        mixed,
        states.reshape(8, 5, 1, 64, 128),
        xwin.transpose(1, 0, 2),
        bcwin.transpose(1, 0, 2),
    )


def solution(mesh):
    return jax.shard_map(
        local,
        mesh=mesh,
        in_specs=(
            P(None, "tp"), P("tp"), P("tp", "kv"), P("tp", "kv"), P("tp", "kv"), P("tp", "kv"),
            P(None, "kv"), P(None, "kv"), P("kv"), P("kv"), P("kv"), P("kv"), P("kv", None),
            P("tp", None, "kv", None, None), P("tp", None, "kv"), P("tp", None, "kv"), P("tp"),
        ),
        out_specs=(
            P("tp", "kv"), P("tp", None, "kv", None, None), P("tp", None, "kv"), P("tp", None, "kv"),
        ),
        check_vma=False,
    )
```

```python
import jax
import jax.numpy as jnp
from jax import lax
from jax.experimental import pallas as pl
from jax.experimental.pallas import tpu as pltpu
from jax.sharding import PartitionSpec as P

D = 4096
INNER = 8192
EPSILON = 1e-05
MESH = pl.DeviceIdType.MESH
F32 = jnp.float32
BF16 = jnp.bfloat16
SIDE = 8
FAR = (4, 3, 5, 2, 6, 1, 7, 0)
CORNER = [(dz, dy) for dz in FAR[:3] for dy in FAR[:3]]
OTHERS = sorted(
    ((dz, dy) for dz in FAR for dy in FAR if (dz or dy) and (dz, dy) not in CORNER),
    key=lambda p: -(min(p[0], SIDE - p[0]) + min(p[1], SIDE - p[1])),
)


def iota(shape, dim):
    return lax.broadcasted_iota(jnp.int32, shape, dim)


def silu(v):
    return v / (1.0 + jnp.exp(-v))


def softplus(v):
    return jnp.maximum(v, 0.0) + jnp.log1p(jnp.exp(-jnp.abs(v)))


def wait_for(ref, sem):
    pltpu.make_async_copy(ref, ref, sem).wait()


def transpose_blocks(rows):
    lane = iota((8, 128), 1)
    low = lane < 64
    even = lax.rem(lane, 64) < 32
    half = [None] * 4
    for g in range(2):
        near, far = rows[g], rows[g + 2]
        half[g] = jnp.where(low, near, pltpu.roll(far, 64, 1))
        half[g + 2] = jnp.where(low, pltpu.roll(near, 64, 1), far)
    out = []
    for g in (0, 2):
        near, far = half[g], half[g + 1]
        out.append(jnp.where(even, near, pltpu.roll(far, 32, 1)))
        out.append(jnp.where(even, pltpu.roll(near, 96, 1), far))
    return out


def mixer(
    hidden, gain, xw, zw, bcw, dtw, xk, bck, ogain, ow, saved, xh, bch,
    accepted_h, dt_bias, decay_log, skip,
    mixed, states, xwin, bcwin,
    hidden_v, gain_v, wt_v, dt_v, xk_v, bck_v, ogain_v, ow_v, saved_v, xh_v, bch_v,
    hg_v, prod_v, fb_v,
    sa, sb, ra, rb, hs, hr,
    wk, ws, sx, sr, ob, ro, qs, qr, qp, rq, ms,
    accepted, load, sa_s, sb_s, hs_s, ra_s, rb_s, hr_s, ws_s, wr_s, sx_s, sr_s, qs_s, qr_s, ob_s, ro_s, qp_s, rq_s, near, ready,
):
    kv = lax.axis_index("kv")
    tp = lax.axis_index("tp")
    core = lax.rem(kv, 2)
    chip = lax.div(kv, 2)
    y = lax.rem(chip, SIDE)
    z = lax.div(chip, SIDE)
    member = lax.rem(kv, 4)
    base = kv - member

    def at(dz, dy):
        return (lax.rem(z + dz, SIDE) * SIDE + lax.rem(y + dy, SIDE)) * 2 + core

    loads = []

    def fetch(src, dst):
        copy = pltpu.make_async_copy(src, dst, load.at[len(loads)])
        copy.start()
        loads.append(copy)
        return copy

    l_hidden = fetch(hidden, hidden_v)
    l_gain = fetch(gain, gain_v)
    l_dt = fetch(dtw, dt_v)
    l_w = [
        fetch(xw, wt_v.at[pl.ds(0, 64)]),
        fetch(zw, wt_v.at[pl.ds(64, 64)]),
        fetch(bcw, wt_v.at[pl.ds(128, 64)]),
    ]

    barrier = pltpu.get_barrier_semaphore()

    def greet(k, t):
        pl.semaphore_signal(barrier, inc=1, device_id=(k, t), device_id_type=MESH)

    for dt in (2, 1, 3, 0):
        for dm in (2, 3, 1, 0):
            if dm or dt:
                greet(base + lax.rem(member + dm, 4), lax.rem(tp + dt, 4))
    for d in (3, 5, 2, 6, 1, 7):
        greet(at(d, 0), tp)
        greet(at(0, d), tp)

    l_hist = [fetch(accepted_h, accepted), fetch(xh, xh_v), fetch(bch, bch_v), fetch(xk, xk_v), fetch(bck, bck_v)]
    l_saved = fetch(saved, saved_v)
    l_ow = fetch(ow, ow_v)
    l_ogain = fetch(ogain, ogain_v)

    wt_v[pl.ds(192, 64), :] = jnp.zeros((64, 1024), BF16)
    l_gain.wait()
    l_hidden.wait()
    l_dt.wait()
    gains = gain_v[...].astype(F32)
    gain_row = jnp.concatenate([gains[j : j + 1] for j in range(8)], axis=1)
    dt_row = dt_v[...].astype(F32)
    squares, dts = [], []
    for i in range(4):
        wide = hidden_v[pl.ds(32 * i, 32), :].astype(F32)
        squares.append(jnp.sum(wide * wide, axis=1, keepdims=True))
        gained = (wide * gain_row).astype(BF16)
        hg_v[pl.ds(32 * i, 32), :] = gained
        dts.append(jnp.sum(gained.astype(F32) * dt_row, axis=1, keepdims=True))
    for copy in l_w:
        copy.wait()
    product = lax.dot_general(
        hg_v[...], wt_v[...], (((1,), (1,)), ((), ())), preferred_element_type=F32
    )
    lane32 = iota((32, 128), 1)
    prod_v[0] = product[:, 0:128]
    for i in range(4):
        high = squares[i].astype(BF16).astype(F32)
        tail = product[32 * i : 32 * i + 32, 128:256]
        tail = jnp.where(lane32 == 64, dts[i], tail)
        tail = jnp.where(lane32 == 65, high, tail)
        tail = jnp.where(lane32 == 66, squares[i] - high, tail)
        prod_v[1, pl.ds(32 * i, 32), :] = tail
    lane = iota((8, 128), 1)
    low = lane < 64
    for i in range(4):
        rows = [prod_v[0, pl.ds(32 * i + t, 8, stride=4), :] for t in range(4)]
        tails = [prod_v[1, pl.ds(32 * i + t, 8, stride=4), :] for t in range(4)]
        misc = tails[0]
        for t in range(1, 4):
            misc = jnp.where(lane < 64 + 4 * t, misc, pltpu.roll(tails[t], 4 * t, 1))
        sa[i] = jnp.concatenate([*rows, misc], axis=0).astype(BF16)
        sb[i] = jnp.concatenate(
            [jnp.where(low, tails[t], pltpu.roll(tails[t + 1], 64, 1)) for t in (0, 2)], axis=0
        ).astype(BF16)

    for copy in l_hist:
        copy.wait()
    seq = iota((8, 64), 0)
    acc = jnp.zeros((8, 64), jnp.int32)
    for s in range(8):
        acc = jnp.where(seq == s, accepted[s], acc)

    def kept(history):
        wide = [history[i].astype(F32) for i in range(7)]
        out = []
        for j in range(3):
            row = wide[j]
            for k in range(1, 5):
                row = jnp.where(acc == k, wide[j + k], row)
            out.append(row)
        return out

    x_kept = kept(xh_v)
    bc_kept = kept(bch_v)
    packed = jnp.concatenate([*bc_kept, bck_v[...].astype(F32), jnp.zeros((4, 64), F32)], axis=0)
    packed = jnp.concatenate([packed, jnp.zeros((32, 64), F32)], axis=1).astype(BF16)
    hs[...] = packed
    hr[member] = packed
    rb[4 * member] = sb[tp]

    pl.semaphore_wait(barrier, 27)

    def tell(sem, k):
        pl.semaphore_signal(sem, inc=1, device_id=(k, tp), device_id_type=MESH)

    tell(near, at(7, 0))
    tell(near, at(0, 7))
    def send(src, dst, send_sem, recv_sem, k, t):
        copy = pltpu.make_async_remote_copy(
            src_ref=src,
            dst_ref=dst,
            send_sem=send_sem,
            recv_sem=recv_sem,
            device_id=(k, t),
            device_id_type=MESH,
        )
        copy.start()
        return copy

    for dt in (2, 1, 3, 0):
        to_t = lax.rem(tp + dt, 4)
        for dm in (2, 3, 1, 0):
            to_k = base + lax.rem(member + dm, 4)
            if dm or dt:
                send(sb.at[to_t], rb.at[4 * member + (4 - dt) % 4], sb_s, rb_s, to_k, to_t)
        if dt:
            send(sa.at[to_t], ra.at[4 - dt], sa_s, ra_s, kv, to_t)
    for dm in (2, 3, 1):
        send(hs, hr.at[member], hs_s, hr_s, base + lax.rem(member + dm, 4), tp)

    l_saved.wait()
    for s in range(8):
        first = saved_v[s, accepted[s]]
        states[s, 0] = first
        fb_v[pl.ds(64 * s, 64), :] = first.astype(BF16)
    l_ogain.wait()
    l_ow.wait()
    quarter = lax.div(iota((64, 128), 1), 32)
    flip = core == 1
    for i in range(16):
        left = ow_v[:, 256 * i : 256 * i + 128].astype(F32)
        right = ow_v[:, 256 * i + 128 : 256 * i + 256].astype(F32)
        left_64, right_32 = pltpu.roll(left, 64, 1), pltpu.roll(right, 32, 1)
        left_96, right_64 = pltpu.roll(left, 96, 1), pltpu.roll(right, 64, 1)
        first = jnp.where(quarter < 2, jnp.where(quarter == 0, left, left_96), jnp.where(quarter == 2, right_64, right_32))
        second = jnp.where(quarter < 2, jnp.where(quarter == 0, left_96, left_64), jnp.where(quarter == 2, right_32, right))
        wk[0:64, 128 * i : 128 * i + 128] = jnp.where(flip, second, first).astype(BF16)
        ws[:, 128 * i : 128 * i + 128] = jnp.where(flip, first, second).astype(BF16)
    partner = kv + 1 - 2 * core
    send(ws, wk.at[pl.ds(64, 64)], ws_s, wr_s, partner, tp)
    pl.semaphore_wait(near, 2)
    for d in FAR[:-1]:
        tell(ready, at(d, 0))

    wait_for(ra.at[pl.ds(1, 3)], ra_s)
    wait_for(rb.at[pl.ds(0, 15)], rb_s)
    wait_for(hr.at[pl.ds(0, 3)], hr_s)

    def total(blocks):
        out = blocks[0].astype(F32)
        for block in blocks[1:]:
            out = out + block.astype(F32)
        return out

    def pieces(value):
        return [value[8 * t : 8 * t + 8] for t in range(4)]

    def spread(value, at):
        return jnp.broadcast_to(value[:, at : at + 1], (8, 128))

    def rounded(value):
        return value.astype(BF16).astype(F32)

    wide = total([sa[tp]] + [ra[i] for i in range(1, 4)])
    misc = wide[32:40]
    scales = lax.rsqrt((misc + pltpu.roll(misc, 127, 1)) / D + EPSILON)
    dt_fresh = rounded(misc * pltpu.roll(scales, 127, 1))
    scale = [spread(scales, 65 + 4 * t) for t in range(4)]
    xz = [rounded(wide[8 * t : 8 * t + 8] * scale[t]) for t in range(4)]
    fresh = [total([rb[4 * m + i] for i in range(4)]) for m in range(4)]
    stored = [hr[m].astype(F32)[:, 0:64] for m in range(4)]

    def conv(rows, taps):
        out = []
        for t in range(4):
            value = rows[t] * taps[0:1]
            for j in range(1, 4):
                value = value + rows[t + j] * taps[j : j + 1]
            out.append(silu(value))
        return out

    x_rows = x_kept + [value[:, 0:64] for value in xz]
    x_conv = conv(x_rows, xk_v[...].astype(F32))
    terms = []
    for left, right in ((0, 1), (2, 3)):
        new = []
        for t in (0, 2):
            near, far = (fresh[m][4 * t : 4 * t + 8] for m in (left, right))
            new.append(jnp.where(low, near, pltpu.roll(far, 64, 1)))
            new.append(jnp.where(low, pltpu.roll(near, 64, 1), far))
        new = [rounded(new[t] * scale[t]) for t in range(4)]
        old = jnp.concatenate([stored[left], stored[right]], axis=1)
        terms.append(conv(pieces(old)[:3] + new, old[24:28]))
    b_terms, c_terms = terms

    rate = jnp.exp(jnp.full((8, 128), decay_log[0], F32))
    all_steps = softplus(dt_fresh + dt_bias[0])
    steps = [spread(all_steps, 64 + 4 * t) for t in range(4)]
    cumulated = []
    for t in range(4):
        value = -rate * steps[t]
        cumulated.append(value if t == 0 else cumulated[-1] + value)

    reads = lax.dot_general(
        jnp.concatenate(c_terms, axis=0).astype(BF16),
        fb_v[...],
        (((1,), (1,)), ((), ())),
        preferred_element_type=F32,
    )
    which = lax.rem(iota((32, 128), 0), 8) - jnp.where(lane32 < 64, 0, 1)
    picked = jnp.where(which == 0, reads[:, 0:128], 0.0)
    for i in range(1, 4):
        picked = picked + jnp.where(which == 2 * i, reads[:, 128 * i : 128 * i + 128], 0.0)
    first_part = pieces(picked[:, 0:64] + picked[:, 64:128])

    gated = []
    z_rows = [value[:, 64:128] for value in xz]
    for t in range(4):
        value = jnp.exp(cumulated[t])[:, 0:64] * first_part[t] + skip[0] * x_conv[t]
        for r in range(t + 1):
            weight = jnp.exp(cumulated[t] - cumulated[r]) * steps[r] if r < t else steps[r]
            inner = jnp.sum(c_terms[t] * b_terms[r], axis=1, keepdims=True)
            value = value + weight[:, 0:64] * inner * x_conv[r]
        gated.append(value * silu(z_rows[t]))
    gated = jnp.concatenate(gated, axis=0)
    scaled = (gated * ogain_v[...].astype(F32)).astype(BF16)
    sx[...] = jnp.concatenate([scaled, jnp.zeros((32, 64), BF16)], axis=1)
    send(sx, sr, sx_s, sr_s, partner, tp)
    square_sum = jnp.sum(gated * gated, axis=1, keepdims=True)
    diagonal = iota((32, 128), 0) == lane32
    qs[...] = jnp.sum(jnp.where(diagonal, square_sum, 0.0), axis=0, keepdims=True)
    pl.semaphore_wait(ready, SIDE - 1)
    for dz, dy in CORNER + OTHERS:
        send(qs, rq.at[dz * SIDE + dy], qs_s, rq_s, at(dz, dy), tp)

    wait_for(wk.at[pl.ds(64, 64)], wr_s)
    wait_for(sr, sr_s)

    rows = jnp.concatenate([scaled, sr[:, 0:64]], axis=1)

    def multiply(i):
        start = pl.multiple_of(lax.rem(z + FAR[i], SIDE) * 256, 256)
        partial = jnp.dot(rows, wk[:, pl.ds(start, 256)], preferred_element_type=F32)
        for j in range(2):
            blocks = transpose_blocks(pieces(partial[:, 128 * j : 128 * j + 128]))
            for b in range(4):
                ob[i, 4 * j + b] = blocks[b].astype(BF16)

    def spread_out(dz, dy):
        block = ob.at[FAR.index(dz), lax.rem(y + dy, SIDE)]
        send(block, ro.at[dz * SIDE + dy], ob_s, ro_s, at(dz, dy), tp)

    for i in range(3):
        multiply(i)
    for dz, dy in CORNER:
        spread_out(dz, dy)
    for i in range(3, SIDE):
        multiply(i)
    for dz, dy in OTHERS:
        spread_out(dz, dy)

    x_in = jnp.concatenate([x_conv[t] * steps[t][:, 0:64] for t in range(4)], axis=0)
    x_cols = jnp.transpose(jnp.concatenate([x_in, jnp.zeros((32, 64), F32)], axis=1))
    decays = [jnp.exp(-rate * steps[t]) for t in range(4)]
    for s in range(8):
        state = saved_v[s, accepted[s]]
        for t in range(4):
            i = 8 * t + s
            state = state * decays[t][s : s + 1] + x_cols[0:64, i : i + 1] * b_terms[t][s : s + 1]
            states[s, t + 1] = state
    for j in range(7):
        xwin[j] = x_rows[j].astype(BF16)
    own = total([rb[4 * member + i] for i in range(4)])
    bc_rows = list(bc_kept)
    for t in range(4):
        half = own[8 * (t // 2) : 8 * (t // 2) + 8, 64 * (t % 2) : 64 * (t % 2) + 64]
        bc_rows.append(rounded(half * scale[t][:, 0:64]))
    for j in range(7):
        bcwin[j] = bc_rows[j].astype(BF16)

    wait_for(rq.at[pl.ds(1, 63)], rq_s)
    qp[...] = qs[...] + jnp.sum(rq[pl.ds(1, 63)], axis=0)
    send(qp, qr, qp_s, qr_s, partner, tp)
    wait_for(ro.at[pl.ds(1, 63)], ro_s)
    summed = ob[7, y].astype(F32) + jnp.sum(ro[pl.ds(1, 63)].astype(F32), axis=0)
    wait_for(qr, qr_s)
    squares_row = qp[...] + qr[...]
    column = jnp.sum(jnp.where(diagonal, squares_row, 0.0), axis=1, keepdims=True)
    factor = lax.rsqrt(column / INNER + EPSILON)
    for t in range(4):
        shifted = pltpu.roll(summed, (128 - 32 * t) % 128, 1) if t else summed
        ms[pl.ds(t, 8, stride=4), :] = shifted * factor[8 * t : 8 * t + 8]
    mixed[...] = ms[:, 0:32].astype(BF16)

    wait_for(sa.at[pl.ds(0, 3)], sa_s)
    wait_for(rb.at[pl.ds(0, 15)], sb_s)
    wait_for(hr.at[pl.ds(0, 3)], hs_s)
    wait_for(ws, ws_s)
    wait_for(sx, sx_s)
    wait_for(rq.at[pl.ds(1, 63)], qs_s)
    wait_for(ro.at[pl.ds(1, 63)], ob_s)
    wait_for(qp, qp_s)


def writer(mixed, states, xwin, bcwin, mixed_o, states_o, xwin_o, bcwin_o, sem):
    copies = [
        pltpu.make_async_copy(states.at[pl.ds(2 * i, 2)], states_o.at[pl.ds(2 * i, 2)], sem.at[i])
        for i in range(4)
    ]
    copies.append(pltpu.make_async_copy(mixed, mixed_o, sem.at[4]))
    copies.append(pltpu.make_async_copy(xwin, xwin_o, sem.at[5]))
    copies.append(pltpu.make_async_copy(bcwin, bcwin_o, sem.at[6]))
    for copy in copies:
        copy.start()
    for copy in copies:
        copy.wait()


def local(
    hidden, input_gain, x_weight, z_weight, bc_weight, dt_weight, x_kernel, bc_kernel,
    dt_bias, decay_log, skip_scale, output_gain, output_weight, saved_states, x_history,
    bc_history, accepted,
):
    shapes = [((32, 32), BF16), ((8, 5, 64, 128), F32), ((7, 8, 64), BF16), ((7, 8, 64), BF16)]
    hbm = pl.BlockSpec(memory_space=pltpu.HBM)
    smem = pl.BlockSpec(memory_space=pltpu.SMEM)
    vmem = pl.BlockSpec(memory_space=pltpu.VMEM)
    dma = pltpu.SemaphoreType.DMA
    scratch = [
        ((128, 1024), BF16), ((8, 128), BF16), ((256, 1024), BF16), ((1, 1024), BF16),
        ((4, 64), BF16), ((4, 64), BF16), ((1, 64), BF16), ((64, 4096), BF16),
        ((8, 5, 64, 128), F32), ((7, 8, 64), BF16), ((7, 8, 64), BF16),
        ((128, 1024), BF16), ((2, 128, 128), F32), ((512, 128), BF16),
        ((4, 40, 128), BF16), ((4, 16, 128), BF16), ((4, 40, 128), BF16), ((16, 16, 128), BF16),
        ((32, 128), BF16), ((4, 32, 128), BF16),
        ((128, 2048), BF16), ((64, 2048), BF16), ((32, 128), BF16), ((32, 128), BF16),
        ((8, 8, 8, 128), BF16), ((64, 8, 128), BF16),
        ((1, 128), F32), ((1, 128), F32), ((1, 128), F32), ((64, 1, 128), F32), ((32, 128), F32),
    ]
    args = [
        hidden, input_gain.reshape(8, 128), x_weight.T, z_weight.T, bc_weight.T, dt_weight.T,
        x_kernel, bc_kernel, output_gain.reshape(1, 64), output_weight,
        saved_states.reshape(8, 5, 64, 128), x_history.transpose(1, 0, 2),
        bc_history.transpose(1, 0, 2), accepted,
    ]
    args = [pltpu.with_memory_space_constraint(arg, pltpu.HBM) for arg in args]
    results = pl.pallas_call(
        mixer,
        name="mixer",
        out_shape=[pltpu.VMEM(shape, dtype) for shape, dtype in shapes],
        in_specs=[hbm] * len(args) + [smem] * 3,
        out_specs=[vmem] * 4,
        scratch_shapes=[pltpu.VMEM(shape, dtype) for shape, dtype in scratch]
        + [pltpu.SMEM((8,), jnp.int32), dma((20,))]
        + [dma(())] * 16
        + [pltpu.SemaphoreType.REGULAR] * 2,
        compiler_params=pltpu.CompilerParams(
            collective_id=0, has_side_effects=True, vmem_limit_bytes=24 << 20
        ),
    )(*args, dt_bias, decay_log, skip_scale)
    mixed, states, xwin, bcwin = pl.pallas_call(
        writer,
        name="writer",
        out_shape=[jax.ShapeDtypeStruct(shape, dtype) for shape, dtype in shapes],
        in_specs=[vmem] * 4,
        out_specs=[hbm] * 4,
        scratch_shapes=[dma((7,))],
        compiler_params=pltpu.CompilerParams(vmem_limit_bytes=8 << 20),
    )(*results)
    return (
        mixed,
        states.reshape(8, 5, 1, 64, 128),
        xwin.transpose(1, 0, 2),
        bcwin.transpose(1, 0, 2),
    )


def solution(mesh):
    return jax.shard_map(
        local,
        mesh=mesh,
        in_specs=(
            P(None, "tp"), P("tp"), P("tp", "kv"), P("tp", "kv"), P("tp", "kv"), P("tp", "kv"),
            P(None, "kv"), P(None, "kv"), P("kv"), P("kv"), P("kv"), P("kv"), P("kv", None),
            P("tp", None, "kv", None, None), P("tp", None, "kv"), P("tp", None, "kv"), P("tp"),
        ),
        out_specs=(
            P("tp", "kv"), P("tp", None, "kv", None, None), P("tp", None, "kv"), P("tp", None, "kv"),
        ),
        check_vma=False,
    )
```

```python
import jax
import jax.numpy as jnp
from jax import lax
from jax.experimental import pallas as pl
from jax.experimental.pallas import tpu as pltpu
from jax.sharding import PartitionSpec as P

D = 4096
INNER = 8192
EPSILON = 1e-05
MESH = pl.DeviceIdType.MESH
F32 = jnp.float32
BF16 = jnp.bfloat16
SIDE = 8
FAR = (4, 3, 5, 2, 6, 1, 7, 0)
ALONG = (1, 4, 2, 3, 5, 6, 7, 0)
EARLY = [(dz, dy) for pair in (ALONG[:2], ALONG[2:4]) for dy in FAR for dz in pair]
LATE = [(dz, dy) for dz in ALONG[4:] for dy in FAR if dz or dy]


def iota(shape, dim):
    return lax.broadcasted_iota(jnp.int32, shape, dim)


def silu(v):
    return v / (1.0 + jnp.exp(-v))


def softplus(v):
    return jnp.maximum(v, 0.0) + jnp.log1p(jnp.exp(-jnp.abs(v)))


def wait_for(ref, sem):
    pltpu.make_async_copy(ref, ref, sem).wait()


def transpose_blocks(rows):
    lane = iota((8, 128), 1)
    low = lane < 64
    even = lax.rem(lane, 64) < 32
    half = [None] * 4
    for g in range(2):
        near, far = rows[g], rows[g + 2]
        half[g] = jnp.where(low, near, pltpu.roll(far, 64, 1))
        half[g + 2] = jnp.where(low, pltpu.roll(near, 64, 1), far)
    out = []
    for g in (0, 2):
        near, far = half[g], half[g + 1]
        out.append(jnp.where(even, near, pltpu.roll(far, 32, 1)))
        out.append(jnp.where(even, pltpu.roll(near, 96, 1), far))
    return out


def mixer(
    hidden, gain, xw, zw, bcw, dtw, xk, bck, ogain, ow, saved, xh, bch,
    accepted_h, dt_bias, decay_log, skip,
    mixed, states, xwin, bcwin,
    hidden_v, gain_v, wt_v, dt_v, xk_v, bck_v, ogain_v, ow_v, saved_v, xh_v, bch_v,
    hg_v, prod_v, fb_v,
    sa, sb, ra, rb, hs, hr,
    wk, ws, sx, sr, ob, ro, qs, qr, qp, rq, ms,
    accepted, load, sa_s, sb_s, hs_s, ra_s, rb_s, hr_s, ws_s, wr_s, sx_s, sr_s, qs_s, qr_s, ob_s, ro_s, qp_s, rq_s, near, ready,
):
    kv = lax.axis_index("kv")
    tp = lax.axis_index("tp")
    core = lax.rem(kv, 2)
    chip = lax.div(kv, 2)
    y = lax.rem(chip, SIDE)
    z = lax.div(chip, SIDE)
    member = lax.rem(kv, 4)
    base = kv - member

    def at(dz, dy):
        return (lax.rem(z + dz, SIDE) * SIDE + lax.rem(y + dy, SIDE)) * 2 + core

    loads = []

    def fetch(src, dst):
        copy = pltpu.make_async_copy(src, dst, load.at[len(loads)])
        copy.start()
        loads.append(copy)
        return copy

    l_hidden = fetch(hidden, hidden_v)
    l_gain = fetch(gain, gain_v)
    l_dt = fetch(dtw, dt_v)
    l_w = [
        fetch(xw, wt_v.at[pl.ds(0, 64)]),
        fetch(zw, wt_v.at[pl.ds(64, 64)]),
        fetch(bcw, wt_v.at[pl.ds(128, 64)]),
    ]

    barrier = pltpu.get_barrier_semaphore()

    def greet(k, t):
        pl.semaphore_signal(barrier, inc=1, device_id=(k, t), device_id_type=MESH)

    for dt in (2, 1, 3, 0):
        for dm in (2, 3, 1, 0):
            if dm or dt:
                greet(base + lax.rem(member + dm, 4), lax.rem(tp + dt, 4))
    for d in (3, 5, 2, 6, 1, 7):
        greet(at(d, 0), tp)
        greet(at(0, d), tp)

    l_hist = [fetch(accepted_h, accepted), fetch(xh, xh_v), fetch(bch, bch_v), fetch(xk, xk_v), fetch(bck, bck_v)]
    l_saved = fetch(saved, saved_v)
    l_ow = fetch(ow, ow_v)
    l_ogain = fetch(ogain, ogain_v)

    wt_v[pl.ds(192, 64), :] = jnp.zeros((64, 1024), BF16)
    l_gain.wait()
    l_hidden.wait()
    l_dt.wait()
    gains = gain_v[...].astype(F32)
    gain_row = jnp.concatenate([gains[j : j + 1] for j in range(8)], axis=1)
    dt_row = dt_v[...].astype(F32)
    squares, dts = [], []
    for i in range(4):
        wide = hidden_v[pl.ds(32 * i, 32), :].astype(F32)
        squares.append(jnp.sum(wide * wide, axis=1, keepdims=True))
        gained = (wide * gain_row).astype(BF16)
        hg_v[pl.ds(32 * i, 32), :] = gained
        dts.append(jnp.sum(gained.astype(F32) * dt_row, axis=1, keepdims=True))
    for copy in l_w:
        copy.wait()
    product = lax.dot_general(
        hg_v[...], wt_v[...], (((1,), (1,)), ((), ())), preferred_element_type=F32
    )
    lane32 = iota((32, 128), 1)
    prod_v[0] = product[:, 0:128]
    for i in range(4):
        high = squares[i].astype(BF16).astype(F32)
        tail = product[32 * i : 32 * i + 32, 128:256]
        tail = jnp.where(lane32 == 64, dts[i], tail)
        tail = jnp.where(lane32 == 65, high, tail)
        tail = jnp.where(lane32 == 66, squares[i] - high, tail)
        prod_v[1, pl.ds(32 * i, 32), :] = tail
    lane = iota((8, 128), 1)
    low = lane < 64
    for i in range(4):
        rows = [prod_v[0, pl.ds(32 * i + t, 8, stride=4), :] for t in range(4)]
        tails = [prod_v[1, pl.ds(32 * i + t, 8, stride=4), :] for t in range(4)]
        misc = tails[0]
        for t in range(1, 4):
            misc = jnp.where(lane < 64 + 4 * t, misc, pltpu.roll(tails[t], 4 * t, 1))
        sa[i] = jnp.concatenate([*rows, misc], axis=0).astype(BF16)
        sb[i] = jnp.concatenate(
            [jnp.where(low, tails[t], pltpu.roll(tails[t + 1], 64, 1)) for t in (0, 2)], axis=0
        ).astype(BF16)

    for copy in l_hist:
        copy.wait()
    seq = iota((8, 64), 0)
    acc = jnp.zeros((8, 64), jnp.int32)
    for s in range(8):
        acc = jnp.where(seq == s, accepted[s], acc)

    def kept(history):
        wide = [history[i].astype(F32) for i in range(7)]
        out = []
        for j in range(3):
            row = wide[j]
            for k in range(1, 5):
                row = jnp.where(acc == k, wide[j + k], row)
            out.append(row)
        return out

    x_kept = kept(xh_v)
    bc_kept = kept(bch_v)
    packed = jnp.concatenate([*bc_kept, bck_v[...].astype(F32), jnp.zeros((4, 64), F32)], axis=0)
    packed = jnp.concatenate([packed, jnp.zeros((32, 64), F32)], axis=1).astype(BF16)
    hs[...] = packed
    hr[member] = packed
    rb[4 * member] = sb[tp]

    pl.semaphore_wait(barrier, 27)

    def tell(sem, k):
        pl.semaphore_signal(sem, inc=1, device_id=(k, tp), device_id_type=MESH)

    tell(near, at(7, 0))
    tell(near, at(0, 7))
    def send(src, dst, send_sem, recv_sem, k, t):
        copy = pltpu.make_async_remote_copy(
            src_ref=src,
            dst_ref=dst,
            send_sem=send_sem,
            recv_sem=recv_sem,
            device_id=(k, t),
            device_id_type=MESH,
        )
        copy.start()
        return copy

    for dt in (2, 1, 3, 0):
        to_t = lax.rem(tp + dt, 4)
        for dm in (2, 3, 1, 0):
            to_k = base + lax.rem(member + dm, 4)
            if dm or dt:
                send(sb.at[to_t], rb.at[4 * member + (4 - dt) % 4], sb_s, rb_s, to_k, to_t)
        if dt:
            send(sa.at[to_t], ra.at[4 - dt], sa_s, ra_s, kv, to_t)
    for dm in (2, 3, 1):
        send(hs, hr.at[member], hs_s, hr_s, base + lax.rem(member + dm, 4), tp)

    l_saved.wait()
    for s in range(8):
        first = saved_v[s, accepted[s]]
        states[s, 0] = first
        fb_v[pl.ds(64 * s, 64), :] = first.astype(BF16)
    l_ogain.wait()
    l_ow.wait()
    quarter = lax.div(iota((64, 128), 1), 32)
    flip = core == 1
    for i in range(16):
        left = ow_v[:, 256 * i : 256 * i + 128].astype(F32)
        right = ow_v[:, 256 * i + 128 : 256 * i + 256].astype(F32)
        left_64, right_32 = pltpu.roll(left, 64, 1), pltpu.roll(right, 32, 1)
        left_96, right_64 = pltpu.roll(left, 96, 1), pltpu.roll(right, 64, 1)
        first = jnp.where(quarter < 2, jnp.where(quarter == 0, left, left_96), jnp.where(quarter == 2, right_64, right_32))
        second = jnp.where(quarter < 2, jnp.where(quarter == 0, left_96, left_64), jnp.where(quarter == 2, right_32, right))
        wk[0:64, 128 * i : 128 * i + 128] = jnp.where(flip, second, first).astype(BF16)
        ws[:, 128 * i : 128 * i + 128] = jnp.where(flip, first, second).astype(BF16)
    partner = kv + 1 - 2 * core
    send(ws, wk.at[pl.ds(64, 64)], ws_s, wr_s, partner, tp)
    pl.semaphore_wait(near, 2)
    for d in FAR[:-1]:
        tell(ready, at(d, 0))

    wait_for(ra.at[pl.ds(1, 3)], ra_s)
    wait_for(rb.at[pl.ds(0, 15)], rb_s)
    wait_for(hr.at[pl.ds(0, 3)], hr_s)

    def total(blocks):
        out = blocks[0].astype(F32)
        for block in blocks[1:]:
            out = out + block.astype(F32)
        return out

    def pieces(value):
        return [value[8 * t : 8 * t + 8] for t in range(4)]

    def spread(value, at):
        return jnp.broadcast_to(value[:, at : at + 1], (8, 128))

    def rounded(value):
        return value.astype(BF16).astype(F32)

    wide = total([sa[tp]] + [ra[i] for i in range(1, 4)])
    misc = wide[32:40]
    scales = lax.rsqrt((misc + pltpu.roll(misc, 127, 1)) / D + EPSILON)
    dt_fresh = rounded(misc * pltpu.roll(scales, 127, 1))
    scale = [spread(scales, 65 + 4 * t) for t in range(4)]
    xz = [rounded(wide[8 * t : 8 * t + 8] * scale[t]) for t in range(4)]
    fresh = [total([rb[4 * m + i] for i in range(4)]) for m in range(4)]
    stored = [hr[m].astype(F32)[:, 0:64] for m in range(4)]

    def conv(rows, taps):
        out = []
        for t in range(4):
            value = rows[t] * taps[0:1]
            for j in range(1, 4):
                value = value + rows[t + j] * taps[j : j + 1]
            out.append(silu(value))
        return out

    x_rows = x_kept + [value[:, 0:64] for value in xz]
    x_conv = conv(x_rows, xk_v[...].astype(F32))
    terms = []
    for left, right in ((0, 1), (2, 3)):
        new = []
        for t in (0, 2):
            near, far = (fresh[m][4 * t : 4 * t + 8] for m in (left, right))
            new.append(jnp.where(low, near, pltpu.roll(far, 64, 1)))
            new.append(jnp.where(low, pltpu.roll(near, 64, 1), far))
        new = [rounded(new[t] * scale[t]) for t in range(4)]
        old = jnp.concatenate([stored[left], stored[right]], axis=1)
        terms.append(conv(pieces(old)[:3] + new, old[24:28]))
    b_terms, c_terms = terms

    rate = jnp.exp(jnp.full((8, 128), decay_log[0], F32))
    all_steps = softplus(dt_fresh + dt_bias[0])
    steps = [spread(all_steps, 64 + 4 * t) for t in range(4)]
    cumulated = []
    for t in range(4):
        value = -rate * steps[t]
        cumulated.append(value if t == 0 else cumulated[-1] + value)

    reads = lax.dot_general(
        jnp.concatenate(c_terms, axis=0).astype(BF16),
        fb_v[...],
        (((1,), (1,)), ((), ())),
        preferred_element_type=F32,
    )
    which = lax.rem(iota((32, 128), 0), 8) - jnp.where(lane32 < 64, 0, 1)
    picked = jnp.where(which == 0, reads[:, 0:128], 0.0)
    for i in range(1, 4):
        picked = picked + jnp.where(which == 2 * i, reads[:, 128 * i : 128 * i + 128], 0.0)
    first_part = pieces(picked[:, 0:64] + picked[:, 64:128])

    gated = []
    z_rows = [value[:, 64:128] for value in xz]
    for t in range(4):
        value = jnp.exp(cumulated[t])[:, 0:64] * first_part[t] + skip[0] * x_conv[t]
        for r in range(t + 1):
            weight = jnp.exp(cumulated[t] - cumulated[r]) * steps[r] if r < t else steps[r]
            inner = jnp.sum(c_terms[t] * b_terms[r], axis=1, keepdims=True)
            value = value + weight[:, 0:64] * inner * x_conv[r]
        gated.append(value * silu(z_rows[t]))
    gated = jnp.concatenate(gated, axis=0)
    scaled = (gated * ogain_v[...].astype(F32)).astype(BF16)
    sx[...] = jnp.concatenate([scaled, jnp.zeros((32, 64), BF16)], axis=1)
    send(sx, sr, sx_s, sr_s, partner, tp)
    square_sum = jnp.sum(gated * gated, axis=1, keepdims=True)
    diagonal = iota((32, 128), 0) == lane32
    qs[...] = jnp.sum(jnp.where(diagonal, square_sum, 0.0), axis=0, keepdims=True)
    send(qs, qr, qs_s, qr_s, partner, tp)
    pl.semaphore_wait(ready, SIDE - 1)

    wait_for(qr, qr_s)
    qp[...] = qs[...] + qr[...]
    wait_for(wk.at[pl.ds(64, 64)], wr_s)
    wait_for(sr, sr_s)

    rows = jnp.concatenate([scaled, sr[:, 0:64]], axis=1)

    def multiply(i):
        start = pl.multiple_of(lax.rem(z + ALONG[i], SIDE) * 256, 256)
        partial = jnp.dot(rows, wk[:, pl.ds(start, 256)], preferred_element_type=F32)
        for j in range(2):
            blocks = transpose_blocks(pieces(partial[:, 128 * j : 128 * j + 128]))
            for b in range(4):
                ob[i, 4 * j + b] = blocks[b].astype(BF16)

    def spread_out(dz, dy):
        to = at(dz, dy)
        slot = dz * SIDE + dy
        send(ob.at[ALONG.index(dz), lax.rem(y + dy, SIDE)], ro.at[slot], ob_s, ro_s, to, tp)
        send(qp, rq.at[slot], qp_s, rq_s, to, tp)

    for i in range(4):
        multiply(i)
    for dz, dy in EARLY:
        spread_out(dz, dy)
    for i in range(4, SIDE):
        multiply(i)
    for dz, dy in LATE:
        spread_out(dz, dy)

    x_in = jnp.concatenate([x_conv[t] * steps[t][:, 0:64] for t in range(4)], axis=0)
    x_cols = jnp.transpose(jnp.concatenate([x_in, jnp.zeros((32, 64), F32)], axis=1))
    decays = [jnp.exp(-rate * steps[t]) for t in range(4)]
    for s in range(8):
        state = saved_v[s, accepted[s]]
        for t in range(4):
            i = 8 * t + s
            state = state * decays[t][s : s + 1] + x_cols[0:64, i : i + 1] * b_terms[t][s : s + 1]
            states[s, t + 1] = state
    for j in range(7):
        xwin[j] = x_rows[j].astype(BF16)
    own = total([rb[4 * member + i] for i in range(4)])
    bc_rows = list(bc_kept)
    for t in range(4):
        half = own[8 * (t // 2) : 8 * (t // 2) + 8, 64 * (t % 2) : 64 * (t % 2) + 64]
        bc_rows.append(rounded(half * scale[t][:, 0:64]))
    for j in range(7):
        bcwin[j] = bc_rows[j].astype(BF16)

    wait_for(rq.at[pl.ds(1, 63)], rq_s)
    squares_row = qp[...] + jnp.sum(rq[pl.ds(1, 63)], axis=0)
    column = jnp.sum(jnp.where(diagonal, squares_row, 0.0), axis=1, keepdims=True)
    factor = lax.rsqrt(column / INNER + EPSILON)
    wait_for(ro.at[pl.ds(1, 63)], ro_s)
    summed = ob[7, y].astype(F32) + jnp.sum(ro[pl.ds(1, 63)].astype(F32), axis=0)
    for t in range(4):
        shifted = pltpu.roll(summed, (128 - 32 * t) % 128, 1) if t else summed
        ms[pl.ds(t, 8, stride=4), :] = shifted * factor[8 * t : 8 * t + 8]
    mixed[...] = ms[:, 0:32].astype(BF16)

    wait_for(sa.at[pl.ds(0, 3)], sa_s)
    wait_for(rb.at[pl.ds(0, 15)], sb_s)
    wait_for(hr.at[pl.ds(0, 3)], hs_s)
    wait_for(ws, ws_s)
    wait_for(sx, sx_s)
    wait_for(qs, qs_s)
    wait_for(ro.at[pl.ds(1, 63)], ob_s)
    wait_for(rq.at[pl.ds(1, 63)], qp_s)


def writer(mixed, states, xwin, bcwin, mixed_o, states_o, xwin_o, bcwin_o, sem):
    copies = [
        pltpu.make_async_copy(states.at[pl.ds(2 * i, 2)], states_o.at[pl.ds(2 * i, 2)], sem.at[i])
        for i in range(4)
    ]
    copies.append(pltpu.make_async_copy(mixed, mixed_o, sem.at[4]))
    copies.append(pltpu.make_async_copy(xwin, xwin_o, sem.at[5]))
    copies.append(pltpu.make_async_copy(bcwin, bcwin_o, sem.at[6]))
    for copy in copies:
        copy.start()
    for copy in copies:
        copy.wait()


def local(
    hidden, input_gain, x_weight, z_weight, bc_weight, dt_weight, x_kernel, bc_kernel,
    dt_bias, decay_log, skip_scale, output_gain, output_weight, saved_states, x_history,
    bc_history, accepted,
):
    shapes = [((32, 32), BF16), ((8, 5, 64, 128), F32), ((7, 8, 64), BF16), ((7, 8, 64), BF16)]
    hbm = pl.BlockSpec(memory_space=pltpu.HBM)
    smem = pl.BlockSpec(memory_space=pltpu.SMEM)
    vmem = pl.BlockSpec(memory_space=pltpu.VMEM)
    dma = pltpu.SemaphoreType.DMA
    scratch = [
        ((128, 1024), BF16), ((8, 128), BF16), ((256, 1024), BF16), ((1, 1024), BF16),
        ((4, 64), BF16), ((4, 64), BF16), ((1, 64), BF16), ((64, 4096), BF16),
        ((8, 5, 64, 128), F32), ((7, 8, 64), BF16), ((7, 8, 64), BF16),
        ((128, 1024), BF16), ((2, 128, 128), F32), ((512, 128), BF16),
        ((4, 40, 128), BF16), ((4, 16, 128), BF16), ((4, 40, 128), BF16), ((16, 16, 128), BF16),
        ((32, 128), BF16), ((4, 32, 128), BF16),
        ((128, 2048), BF16), ((64, 2048), BF16), ((32, 128), BF16), ((32, 128), BF16),
        ((8, 8, 8, 128), BF16), ((64, 8, 128), BF16),
        ((1, 128), F32), ((1, 128), F32), ((1, 128), F32), ((64, 1, 128), F32), ((32, 128), F32),
    ]
    args = [
        hidden, input_gain.reshape(8, 128), x_weight.T, z_weight.T, bc_weight.T, dt_weight.T,
        x_kernel, bc_kernel, output_gain.reshape(1, 64), output_weight,
        saved_states.reshape(8, 5, 64, 128), x_history.transpose(1, 0, 2),
        bc_history.transpose(1, 0, 2), accepted,
    ]
    args = [pltpu.with_memory_space_constraint(arg, pltpu.HBM) for arg in args]
    results = pl.pallas_call(
        mixer,
        name="mixer",
        out_shape=[pltpu.VMEM(shape, dtype) for shape, dtype in shapes],
        in_specs=[hbm] * len(args) + [smem] * 3,
        out_specs=[vmem] * 4,
        scratch_shapes=[pltpu.VMEM(shape, dtype) for shape, dtype in scratch]
        + [pltpu.SMEM((8,), jnp.int32), dma((20,))]
        + [dma(())] * 16
        + [pltpu.SemaphoreType.REGULAR] * 2,
        compiler_params=pltpu.CompilerParams(
            collective_id=0, has_side_effects=True, vmem_limit_bytes=24 << 20
        ),
    )(*args, dt_bias, decay_log, skip_scale)
    mixed, states, xwin, bcwin = pl.pallas_call(
        writer,
        name="writer",
        out_shape=[jax.ShapeDtypeStruct(shape, dtype) for shape, dtype in shapes],
        in_specs=[vmem] * 4,
        out_specs=[hbm] * 4,
        scratch_shapes=[dma((7,))],
        compiler_params=pltpu.CompilerParams(vmem_limit_bytes=8 << 20),
    )(*results)
    return (
        mixed,
        states.reshape(8, 5, 1, 64, 128),
        xwin.transpose(1, 0, 2),
        bcwin.transpose(1, 0, 2),
    )


def solution(mesh):
    return jax.shard_map(
        local,
        mesh=mesh,
        in_specs=(
            P(None, "tp"), P("tp"), P("tp", "kv"), P("tp", "kv"), P("tp", "kv"), P("tp", "kv"),
            P(None, "kv"), P(None, "kv"), P("kv"), P("kv"), P("kv"), P("kv"), P("kv", None),
            P("tp", None, "kv", None, None), P("tp", None, "kv"), P("tp", None, "kv"), P("tp"),
        ),
        out_specs=(
            P("tp", "kv"), P("tp", None, "kv", None, None), P("tp", None, "kv"), P("tp", None, "kv"),
        ),
        check_vma=False,
    )
```

```python
import jax
import jax.numpy as jnp
from jax import lax
from jax.experimental import pallas as pl
from jax.experimental.pallas import tpu as pltpu
from jax.sharding import PartitionSpec as P

D = 4096
INNER = 8192
EPSILON = 1e-05
MESH = pl.DeviceIdType.MESH
F32 = jnp.float32
BF16 = jnp.bfloat16
SIDE = 8
FAR = (4, 3, 5, 2, 6, 1, 7, 0)
ALONG = (1, 4, 2, 3, 5, 6, 7, 0)
EARLY = [(dz, dy) for dy in FAR for dz in ALONG[:2]]
LATE = [(dz, dy) for dy in FAR for dz in ALONG[2:] if dz or dy]


def iota(shape, dim):
    return lax.broadcasted_iota(jnp.int32, shape, dim)


def silu(v):
    return v / (1.0 + jnp.exp(-v))


def softplus(v):
    return jnp.maximum(v, 0.0) + jnp.log1p(jnp.exp(-jnp.abs(v)))


def wait_for(ref, sem):
    pltpu.make_async_copy(ref, ref, sem).wait()


def transpose_blocks(rows):
    lane = iota((8, 128), 1)
    low = lane < 64
    even = lax.rem(lane, 64) < 32
    half = [None] * 4
    for g in range(2):
        near, far = rows[g], rows[g + 2]
        half[g] = jnp.where(low, near, pltpu.roll(far, 64, 1))
        half[g + 2] = jnp.where(low, pltpu.roll(near, 64, 1), far)
    out = []
    for g in (0, 2):
        near, far = half[g], half[g + 1]
        out.append(jnp.where(even, near, pltpu.roll(far, 32, 1)))
        out.append(jnp.where(even, pltpu.roll(near, 96, 1), far))
    return out


def mixer(
    hidden, gain, xw, zw, bcw, dtw, xk, bck, ogain, ow, saved, xh, bch,
    accepted_h, dt_bias, decay_log, skip,
    mixed, states, xwin, bcwin,
    hidden_v, gain_v, wt_v, dt_v, xk_v, bck_v, ogain_v, ow_v, saved_v, xh_v, bch_v,
    hg_v, prod_v, fb_v,
    sa, sb, ra, rb, hs, hr,
    wk, ws, sx, sr, ob, ro, qs, qr, qp, rq, ms,
    accepted, load, sa_s, sb_s, hs_s, ra_s, rb_s, hr_s, ws_s, wr_s, sx_s, sr_s, qs_s, qr_s, ob_s, ro_s, qp_s, rq_s, near, ready,
):
    kv = lax.axis_index("kv")
    tp = lax.axis_index("tp")
    core = lax.rem(kv, 2)
    chip = lax.div(kv, 2)
    y = lax.rem(chip, SIDE)
    z = lax.div(chip, SIDE)
    member = lax.rem(kv, 4)
    base = kv - member

    def at(dz, dy):
        return (lax.rem(z + dz, SIDE) * SIDE + lax.rem(y + dy, SIDE)) * 2 + core

    loads = []

    def fetch(src, dst):
        copy = pltpu.make_async_copy(src, dst, load.at[len(loads)])
        copy.start()
        loads.append(copy)
        return copy

    l_hidden = fetch(hidden, hidden_v)
    l_gain = fetch(gain, gain_v)
    l_dt = fetch(dtw, dt_v)
    l_w = [
        fetch(xw, wt_v.at[pl.ds(0, 64)]),
        fetch(zw, wt_v.at[pl.ds(64, 64)]),
        fetch(bcw, wt_v.at[pl.ds(128, 64)]),
    ]

    barrier = pltpu.get_barrier_semaphore()

    def greet(k, t):
        pl.semaphore_signal(barrier, inc=1, device_id=(k, t), device_id_type=MESH)

    for dt in (2, 1, 3, 0):
        for dm in (2, 3, 1, 0):
            if dm or dt:
                greet(base + lax.rem(member + dm, 4), lax.rem(tp + dt, 4))
    for d in (3, 5, 2, 6, 1, 7):
        greet(at(d, 0), tp)
        greet(at(0, d), tp)

    l_hist = [fetch(accepted_h, accepted), fetch(xh, xh_v), fetch(bch, bch_v), fetch(xk, xk_v), fetch(bck, bck_v)]
    l_saved = fetch(saved, saved_v)
    l_ow = fetch(ow, ow_v)
    l_ogain = fetch(ogain, ogain_v)

    wt_v[pl.ds(192, 64), :] = jnp.zeros((64, 1024), BF16)
    l_gain.wait()
    l_hidden.wait()
    l_dt.wait()
    gains = gain_v[...].astype(F32)
    gain_row = jnp.concatenate([gains[j : j + 1] for j in range(8)], axis=1)
    dt_row = dt_v[...].astype(F32)
    squares, dts = [], []
    for i in range(4):
        wide = hidden_v[pl.ds(32 * i, 32), :].astype(F32)
        squares.append(jnp.sum(wide * wide, axis=1, keepdims=True))
        gained = (wide * gain_row).astype(BF16)
        hg_v[pl.ds(32 * i, 32), :] = gained
        dts.append(jnp.sum(gained.astype(F32) * dt_row, axis=1, keepdims=True))
    for copy in l_w:
        copy.wait()
    product = lax.dot_general(
        hg_v[...], wt_v[...], (((1,), (1,)), ((), ())), preferred_element_type=F32
    )
    lane32 = iota((32, 128), 1)
    prod_v[0] = product[:, 0:128]
    for i in range(4):
        high = squares[i].astype(BF16).astype(F32)
        tail = product[32 * i : 32 * i + 32, 128:256]
        tail = jnp.where(lane32 == 64, dts[i], tail)
        tail = jnp.where(lane32 == 65, high, tail)
        tail = jnp.where(lane32 == 66, squares[i] - high, tail)
        prod_v[1, pl.ds(32 * i, 32), :] = tail
    lane = iota((8, 128), 1)
    low = lane < 64
    for i in range(4):
        rows = [prod_v[0, pl.ds(32 * i + t, 8, stride=4), :] for t in range(4)]
        tails = [prod_v[1, pl.ds(32 * i + t, 8, stride=4), :] for t in range(4)]
        misc = tails[0]
        for t in range(1, 4):
            misc = jnp.where(lane < 64 + 4 * t, misc, pltpu.roll(tails[t], 4 * t, 1))
        sa[i] = jnp.concatenate([*rows, misc], axis=0).astype(BF16)
        sb[i] = jnp.concatenate(
            [jnp.where(low, tails[t], pltpu.roll(tails[t + 1], 64, 1)) for t in (0, 2)], axis=0
        ).astype(BF16)

    for copy in l_hist:
        copy.wait()
    seq = iota((8, 64), 0)
    acc = jnp.zeros((8, 64), jnp.int32)
    for s in range(8):
        acc = jnp.where(seq == s, accepted[s], acc)

    def kept(history):
        wide = [history[i].astype(F32) for i in range(7)]
        out = []
        for j in range(3):
            row = wide[j]
            for k in range(1, 5):
                row = jnp.where(acc == k, wide[j + k], row)
            out.append(row)
        return out

    x_kept = kept(xh_v)
    bc_kept = kept(bch_v)
    packed = jnp.concatenate([*bc_kept, bck_v[...].astype(F32), jnp.zeros((4, 64), F32)], axis=0)
    packed = jnp.concatenate([packed, jnp.zeros((32, 64), F32)], axis=1).astype(BF16)
    hs[...] = packed
    hr[member] = packed
    rb[4 * member] = sb[tp]

    pl.semaphore_wait(barrier, 27)

    def tell(sem, k):
        pl.semaphore_signal(sem, inc=1, device_id=(k, tp), device_id_type=MESH)

    tell(near, at(7, 0))
    tell(near, at(0, 7))
    def send(src, dst, send_sem, recv_sem, k, t):
        copy = pltpu.make_async_remote_copy(
            src_ref=src,
            dst_ref=dst,
            send_sem=send_sem,
            recv_sem=recv_sem,
            device_id=(k, t),
            device_id_type=MESH,
        )
        copy.start()
        return copy

    for dt in (2, 1, 3, 0):
        to_t = lax.rem(tp + dt, 4)
        for dm in (2, 3, 1, 0):
            to_k = base + lax.rem(member + dm, 4)
            if dm or dt:
                send(sb.at[to_t], rb.at[4 * member + (4 - dt) % 4], sb_s, rb_s, to_k, to_t)
        if dt:
            send(sa.at[to_t], ra.at[4 - dt], sa_s, ra_s, kv, to_t)
    for dm in (2, 3, 1):
        send(hs, hr.at[member], hs_s, hr_s, base + lax.rem(member + dm, 4), tp)

    l_saved.wait()
    for s in range(8):
        first = saved_v[s, accepted[s]]
        states[s, 0] = first
        fb_v[pl.ds(64 * s, 64), :] = first.astype(BF16)
    l_ogain.wait()
    l_ow.wait()
    quarter = lax.div(iota((64, 128), 1), 32)
    flip = core == 1
    for i in range(16):
        left = ow_v[:, 256 * i : 256 * i + 128].astype(F32)
        right = ow_v[:, 256 * i + 128 : 256 * i + 256].astype(F32)
        left_64, right_32 = pltpu.roll(left, 64, 1), pltpu.roll(right, 32, 1)
        left_96, right_64 = pltpu.roll(left, 96, 1), pltpu.roll(right, 64, 1)
        first = jnp.where(quarter < 2, jnp.where(quarter == 0, left, left_96), jnp.where(quarter == 2, right_64, right_32))
        second = jnp.where(quarter < 2, jnp.where(quarter == 0, left_96, left_64), jnp.where(quarter == 2, right_32, right))
        wk[0:64, 128 * i : 128 * i + 128] = jnp.where(flip, second, first).astype(BF16)
        ws[:, 128 * i : 128 * i + 128] = jnp.where(flip, first, second).astype(BF16)
    partner = kv + 1 - 2 * core
    send(ws, wk.at[pl.ds(64, 64)], ws_s, wr_s, partner, tp)
    pl.semaphore_wait(near, 2)
    for d in FAR[:-1]:
        tell(ready, at(d, 0))

    wait_for(ra.at[pl.ds(1, 3)], ra_s)
    wait_for(rb.at[pl.ds(0, 15)], rb_s)
    wait_for(hr.at[pl.ds(0, 3)], hr_s)

    def total(blocks):
        out = blocks[0].astype(F32)
        for block in blocks[1:]:
            out = out + block.astype(F32)
        return out

    def pieces(value):
        return [value[8 * t : 8 * t + 8] for t in range(4)]

    def spread(value, at):
        return jnp.broadcast_to(value[:, at : at + 1], (8, 128))

    def rounded(value):
        return value.astype(BF16).astype(F32)

    wide = total([sa[tp]] + [ra[i] for i in range(1, 4)])
    misc = wide[32:40]
    scales = lax.rsqrt((misc + pltpu.roll(misc, 127, 1)) / D + EPSILON)
    dt_fresh = rounded(misc * pltpu.roll(scales, 127, 1))
    scale = [spread(scales, 65 + 4 * t) for t in range(4)]
    xz = [rounded(wide[8 * t : 8 * t + 8] * scale[t]) for t in range(4)]
    fresh = [total([rb[4 * m + i] for i in range(4)]) for m in range(4)]
    stored = [hr[m].astype(F32)[:, 0:64] for m in range(4)]

    def conv(rows, taps):
        out = []
        for t in range(4):
            value = rows[t] * taps[0:1]
            for j in range(1, 4):
                value = value + rows[t + j] * taps[j : j + 1]
            out.append(silu(value))
        return out

    x_rows = x_kept + [value[:, 0:64] for value in xz]
    x_conv = conv(x_rows, xk_v[...].astype(F32))
    terms = []
    for left, right in ((0, 1), (2, 3)):
        new = []
        for t in (0, 2):
            near, far = (fresh[m][4 * t : 4 * t + 8] for m in (left, right))
            new.append(jnp.where(low, near, pltpu.roll(far, 64, 1)))
            new.append(jnp.where(low, pltpu.roll(near, 64, 1), far))
        new = [rounded(new[t] * scale[t]) for t in range(4)]
        old = jnp.concatenate([stored[left], stored[right]], axis=1)
        terms.append(conv(pieces(old)[:3] + new, old[24:28]))
    b_terms, c_terms = terms

    rate = jnp.exp(jnp.full((8, 128), decay_log[0], F32))
    all_steps = softplus(dt_fresh + dt_bias[0])
    steps = [spread(all_steps, 64 + 4 * t) for t in range(4)]
    cumulated = []
    for t in range(4):
        value = -rate * steps[t]
        cumulated.append(value if t == 0 else cumulated[-1] + value)

    reads = lax.dot_general(
        jnp.concatenate(c_terms, axis=0).astype(BF16),
        fb_v[...],
        (((1,), (1,)), ((), ())),
        preferred_element_type=F32,
    )
    which = lax.rem(iota((32, 128), 0), 8) - jnp.where(lane32 < 64, 0, 1)
    picked = jnp.where(which == 0, reads[:, 0:128], 0.0)
    for i in range(1, 4):
        picked = picked + jnp.where(which == 2 * i, reads[:, 128 * i : 128 * i + 128], 0.0)
    first_part = pieces(picked[:, 0:64] + picked[:, 64:128])

    gated = []
    z_rows = [value[:, 64:128] for value in xz]
    for t in range(4):
        value = jnp.exp(cumulated[t])[:, 0:64] * first_part[t] + skip[0] * x_conv[t]
        for r in range(t + 1):
            weight = jnp.exp(cumulated[t] - cumulated[r]) * steps[r] if r < t else steps[r]
            inner = jnp.sum(c_terms[t] * b_terms[r], axis=1, keepdims=True)
            value = value + weight[:, 0:64] * inner * x_conv[r]
        gated.append(value * silu(z_rows[t]))
    gated = jnp.concatenate(gated, axis=0)
    scaled = (gated * ogain_v[...].astype(F32)).astype(BF16)
    sx[...] = jnp.concatenate([scaled, jnp.zeros((32, 64), BF16)], axis=1)
    send(sx, sr, sx_s, sr_s, partner, tp)
    square_sum = jnp.sum(gated * gated, axis=1, keepdims=True)
    diagonal = iota((32, 128), 0) == lane32
    qs[...] = jnp.sum(jnp.where(diagonal, square_sum, 0.0), axis=0, keepdims=True)
    pl.semaphore_wait(ready, SIDE - 1)
    for dz, dy in EARLY + LATE:
        send(qs, rq.at[dz * SIDE + dy], qs_s, rq_s, at(dz, dy), tp)

    wait_for(wk.at[pl.ds(64, 64)], wr_s)
    wait_for(sr, sr_s)

    rows = jnp.concatenate([scaled, sr[:, 0:64]], axis=1)

    def multiply(i):
        start = pl.multiple_of(lax.rem(z + ALONG[i], SIDE) * 256, 256)
        partial = jnp.dot(rows, wk[:, pl.ds(start, 256)], preferred_element_type=F32)
        for j in range(2):
            blocks = transpose_blocks(pieces(partial[:, 128 * j : 128 * j + 128]))
            for b in range(4):
                ob[i, 4 * j + b] = blocks[b].astype(BF16)

    def spread_out(dz, dy):
        block = ob.at[ALONG.index(dz), lax.rem(y + dy, SIDE)]
        send(block, ro.at[dz * SIDE + dy], ob_s, ro_s, at(dz, dy), tp)

    for i in range(2):
        multiply(i)
    for dz, dy in EARLY:
        spread_out(dz, dy)
    for i in range(2, SIDE):
        multiply(i)
    for dz, dy in LATE:
        spread_out(dz, dy)

    x_in = jnp.concatenate([x_conv[t] * steps[t][:, 0:64] for t in range(4)], axis=0)
    x_cols = jnp.transpose(jnp.concatenate([x_in, jnp.zeros((32, 64), F32)], axis=1))
    decays = [jnp.exp(-rate * steps[t]) for t in range(4)]
    for s in range(8):
        state = saved_v[s, accepted[s]]
        for t in range(4):
            i = 8 * t + s
            state = state * decays[t][s : s + 1] + x_cols[0:64, i : i + 1] * b_terms[t][s : s + 1]
            states[s, t + 1] = state
    for j in range(7):
        xwin[j] = x_rows[j].astype(BF16)
    own = total([rb[4 * member + i] for i in range(4)])
    bc_rows = list(bc_kept)
    for t in range(4):
        half = own[8 * (t // 2) : 8 * (t // 2) + 8, 64 * (t % 2) : 64 * (t % 2) + 64]
        bc_rows.append(rounded(half * scale[t][:, 0:64]))
    for j in range(7):
        bcwin[j] = bc_rows[j].astype(BF16)

    wait_for(rq.at[pl.ds(1, 63)], rq_s)
    qp[...] = qs[...] + jnp.sum(rq[pl.ds(1, 63)], axis=0)
    send(qp, qr, qp_s, qr_s, partner, tp)
    wait_for(ro.at[pl.ds(1, 63)], ro_s)
    summed = ob[7, y].astype(F32) + jnp.sum(ro[pl.ds(1, 63)].astype(F32), axis=0)
    wait_for(qr, qr_s)
    squares_row = qp[...] + qr[...]
    column = jnp.sum(jnp.where(diagonal, squares_row, 0.0), axis=1, keepdims=True)
    factor = lax.rsqrt(column / INNER + EPSILON)
    for t in range(4):
        shifted = pltpu.roll(summed, (128 - 32 * t) % 128, 1) if t else summed
        ms[pl.ds(t, 8, stride=4), :] = shifted * factor[8 * t : 8 * t + 8]
    mixed[...] = ms[:, 0:32].astype(BF16)

    wait_for(sa.at[pl.ds(0, 3)], sa_s)
    wait_for(rb.at[pl.ds(0, 15)], sb_s)
    wait_for(hr.at[pl.ds(0, 3)], hs_s)
    wait_for(ws, ws_s)
    wait_for(sx, sx_s)
    wait_for(rq.at[pl.ds(1, 63)], qs_s)
    wait_for(ro.at[pl.ds(1, 63)], ob_s)
    wait_for(qp, qp_s)


def writer(mixed, states, xwin, bcwin, mixed_o, states_o, xwin_o, bcwin_o, sem):
    copies = [
        pltpu.make_async_copy(states.at[pl.ds(2 * i, 2)], states_o.at[pl.ds(2 * i, 2)], sem.at[i])
        for i in range(4)
    ]
    copies.append(pltpu.make_async_copy(mixed, mixed_o, sem.at[4]))
    copies.append(pltpu.make_async_copy(xwin, xwin_o, sem.at[5]))
    copies.append(pltpu.make_async_copy(bcwin, bcwin_o, sem.at[6]))
    for copy in copies:
        copy.start()
    for copy in copies:
        copy.wait()


def local(
    hidden, input_gain, x_weight, z_weight, bc_weight, dt_weight, x_kernel, bc_kernel,
    dt_bias, decay_log, skip_scale, output_gain, output_weight, saved_states, x_history,
    bc_history, accepted,
):
    shapes = [((32, 32), BF16), ((8, 5, 64, 128), F32), ((7, 8, 64), BF16), ((7, 8, 64), BF16)]
    hbm = pl.BlockSpec(memory_space=pltpu.HBM)
    smem = pl.BlockSpec(memory_space=pltpu.SMEM)
    vmem = pl.BlockSpec(memory_space=pltpu.VMEM)
    dma = pltpu.SemaphoreType.DMA
    scratch = [
        ((128, 1024), BF16), ((8, 128), BF16), ((256, 1024), BF16), ((1, 1024), BF16),
        ((4, 64), BF16), ((4, 64), BF16), ((1, 64), BF16), ((64, 4096), BF16),
        ((8, 5, 64, 128), F32), ((7, 8, 64), BF16), ((7, 8, 64), BF16),
        ((128, 1024), BF16), ((2, 128, 128), F32), ((512, 128), BF16),
        ((4, 40, 128), BF16), ((4, 16, 128), BF16), ((4, 40, 128), BF16), ((16, 16, 128), BF16),
        ((32, 128), BF16), ((4, 32, 128), BF16),
        ((128, 2048), BF16), ((64, 2048), BF16), ((32, 128), BF16), ((32, 128), BF16),
        ((8, 8, 8, 128), BF16), ((64, 8, 128), BF16),
        ((1, 128), F32), ((1, 128), F32), ((1, 128), F32), ((64, 1, 128), F32), ((32, 128), F32),
    ]
    args = [
        hidden, input_gain.reshape(8, 128), x_weight.T, z_weight.T, bc_weight.T, dt_weight.T,
        x_kernel, bc_kernel, output_gain.reshape(1, 64), output_weight,
        saved_states.reshape(8, 5, 64, 128), x_history.transpose(1, 0, 2),
        bc_history.transpose(1, 0, 2), accepted,
    ]
    args = [pltpu.with_memory_space_constraint(arg, pltpu.HBM) for arg in args]
    results = pl.pallas_call(
        mixer,
        name="mixer",
        out_shape=[pltpu.VMEM(shape, dtype) for shape, dtype in shapes],
        in_specs=[hbm] * len(args) + [smem] * 3,
        out_specs=[vmem] * 4,
        scratch_shapes=[pltpu.VMEM(shape, dtype) for shape, dtype in scratch]
        + [pltpu.SMEM((8,), jnp.int32), dma((20,))]
        + [dma(())] * 16
        + [pltpu.SemaphoreType.REGULAR] * 2,
        compiler_params=pltpu.CompilerParams(
            collective_id=0, has_side_effects=True, vmem_limit_bytes=24 << 20
        ),
    )(*args, dt_bias, decay_log, skip_scale)
    mixed, states, xwin, bcwin = pl.pallas_call(
        writer,
        name="writer",
        out_shape=[jax.ShapeDtypeStruct(shape, dtype) for shape, dtype in shapes],
        in_specs=[vmem] * 4,
        out_specs=[hbm] * 4,
        scratch_shapes=[dma((7,))],
        compiler_params=pltpu.CompilerParams(vmem_limit_bytes=8 << 20),
    )(*results)
    return (
        mixed,
        states.reshape(8, 5, 1, 64, 128),
        xwin.transpose(1, 0, 2),
        bcwin.transpose(1, 0, 2),
    )


def solution(mesh):
    return jax.shard_map(
        local,
        mesh=mesh,
        in_specs=(
            P(None, "tp"), P("tp"), P("tp", "kv"), P("tp", "kv"), P("tp", "kv"), P("tp", "kv"),
            P(None, "kv"), P(None, "kv"), P("kv"), P("kv"), P("kv"), P("kv"), P("kv", None),
            P("tp", None, "kv", None, None), P("tp", None, "kv"), P("tp", None, "kv"), P("tp"),
        ),
        out_specs=(
            P("tp", "kv"), P("tp", None, "kv", None, None), P("tp", None, "kv"), P("tp", None, "kv"),
        ),
        check_vma=False,
    )
```
